32 devices in a mesh: kv: 8 (over z, x), tp: 4 (over y, core).
Axes of the slice: x: 2, y: 2, z: 4, core: 2. Of those that a mesh axis runs over, the one named last changes fastest.
Arguments:
- tokens: bfloat16 [64, 12, 4096], P(None, None, 'kv'), may hold values from -6 to 6
- parents: int32 [64, 12], P('kv'), may hold values from -1 to 10, as said below
- accepted: int32 [64], P('kv'), may hold values from 0 to 6
- state: float32 [64, 64, 64, 128], P('kv', 'tp'), may hold values from -4 to 4
- conv_x: bfloat16 [64, 3, 4096], P('kv', None, 'tp'), may hold values from -6 to 6
- conv_b: bfloat16 [64, 3, 2048], P('kv', None, 'tp'), may hold values from -6 to 6
- conv_c: bfloat16 [64, 3, 2048], P('kv', None, 'tp'), may hold values from -6 to 6
- path_x: bfloat16 [64, 6, 4096], P('kv', None, 'tp'), may hold values from -6 to 6
- path_b: bfloat16 [64, 6, 2048], P('kv', None, 'tp'), may hold values from -6 to 6
- path_c: bfloat16 [64, 6, 2048], P('kv', None, 'tp'), may hold values from -6 to 6
- path_dt: bfloat16 [64, 6, 64], P('kv', None, 'tp'), may hold values from -6 to 6
- gain_in: float32 [4096], replicated, may hold values from 0.1 to 1.9
- w_x: bfloat16 [4096, 4096], P('kv', 'tp'), may hold values from -0.09375 to 0.09375
- w_z: bfloat16 [4096, 4096], P('kv', 'tp'), may hold values from -0.09375 to 0.09375
- w_b: bfloat16 [4096, 2048], P('kv', 'tp'), may hold values from -0.09375 to 0.09375
- w_c: bfloat16 [4096, 2048], P('kv', 'tp'), may hold values from -0.09375 to 0.09375
- w_dt: bfloat16 [4096, 64], replicated, may hold values from -0.09375 to 0.09375
- dt_bias: float32 [64], P('tp'), may hold values from -2 to 1
- a_log: float32 [64], P('tp'), may hold values from -3 to 1.5
- d_skip: float32 [64], P('tp'), may hold values from 0.5 to 1.5
- conv_wx: bfloat16 [4, 4096], P(None, 'tp'), may hold values from -3 to 3
- conv_wb: bfloat16 [4, 2048], P(None, 'tp'), may hold values from -3 to 3
- conv_wc: bfloat16 [4, 2048], P(None, 'tp'), may hold values from -3 to 3
- gain_out: float32 [4096], P('tp'), may hold values from 0.1 to 1.9
- w_out: bfloat16 [4096, 4096], P('tp', 'kv'), may hold values from -0.09375 to 0.09375
Outputs:
- mixed: bfloat16 [64, 12, 4096], P('kv', None, 'tp')
- new_state: float32 [64, 64, 64, 128], P('kv', 'tp')
The draws below stay inside these ranges and needn't reach their ends.
Inputs may be any that keep to these rules, and one draw needn't show every extreme that they name: `parents`: each proposal's parent is -1 or an earlier proposal of the same sequence; the first proposal's parent is -1.
All inputs are finite; a program needn't handle non-finite values.
Results may differ from the reference program's by a relative error of at most 0.03.
Values may be sent and summed in bfloat16 or wider, within the bound.
No kernel may reach another device: no remote copies, remote signals or barrier semaphores. Data moves between devices by JAX's collectives and lax.ppermute only.
A program may use at most 128 MiB of HBM per device.

```python
import jax
import jax.numpy as jnp
from jax import lax

D = 4096
G = 16
HPG = 4
H = 64
HD = 64
N = 128
INNER = 4096
CONV = 4
Q = 12
P_SIZE = 6
SEQS = 64
N_TP = 4


def draw_parents(key, part):
    jumps = jax.random.randint(key, (SEQS, Q), 0, 3)
    places = jnp.arange(Q, dtype=jnp.int32)[None, :]
    return jnp.maximum(places - 1 - jumps, -1).astype(jnp.int32)


def touch_ends(array, key, low, largest):
    longest = array.shape.index(max(array.shape))
    spots = []
    for shift in (0, 1):
        where = [jax.random.randint(jax.random.fold_in(key, axis), (), 0, length) for axis, length in enumerate(array.shape)]
        where[longest] = (where[longest] + shift) % array.shape[longest]
        spots.append(tuple(where))
    return array.at[spots[0]].set(low).at[spots[1]].set(largest)


def raised(values, stream_key, source, target, shards_of, factor):
    def block_of(position):
        return (jnp.arange(values.shape[position]) // (values.shape[position] // shards_of)).reshape((-1,) + (1,) * (values.ndim - 1 - position))

    near = jax.random.permutation(stream_key, shards_of)[block_of(target)]
    second = (block_of(target) + shards_of // 2) % shards_of
    return jnp.where((block_of(source) == near) | (block_of(source) == second), factor * values, values)


def block_scale(key, extent, split, smallest, high):
    gain = 1.0
    for dim, blocks in split:
        steps = jax.random.uniform(jax.random.fold_in(jax.random.fold_in(key, 6), dim), (blocks,), jnp.float32, smallest / len(split), high / len(split))
        gain = gain * jnp.repeat(jnp.exp(steps), extent[dim] // blocks).reshape((-1,) + (1,) * (len(extent) - 1 - dim))
    return gain


def noise(rng, dims, spread, bound, shards=(), kind=jnp.bfloat16):
    array = jax.random.normal(rng, dims, jnp.float32) * spread
    if len(shards) > 0:
        array = block_scale(rng, dims, shards, -0.22, 0.18) * array
    return jnp.clip(array, min=-bound, max=bound).astype(kind)


def heavy_noise(own_key, shape, deviation, reach, shards, heavy, kind=jnp.bfloat16):
    array = deviation * jax.random.normal(own_key, shape, jnp.float32)
    if shards:
        array = array * block_scale(own_key, shape, shards, -0.22, 0.18)
    return jnp.clip(raised(array, jax.random.fold_in(own_key, 3), *heavy), -reach, reach).astype(kind)


def setup_inputs(seed: int = 0) -> dict:
    key_list = jax.random.split(jax.random.key(seed), 26)
    tokens = heavy_noise(key_list[0], (SEQS, Q, D), 1.0, 6.0, ((2, 8),), (2, 0, 8, 2.0))
    parents = draw_parents(jax.random.fold_in(key_list[25], 71), 0)
    accepted = touch_ends(jax.random.randint(key_list[2], (SEQS,), 0, P_SIZE + 1), jax.random.fold_in(key_list[2], 1), 0, P_SIZE).astype(jnp.int32)
    state = noise(key_list[3], (SEQS, H, HD, N), 0.3, 4.0, ((0, 8), (1, 4)), jnp.float32)
    conv_x = noise(key_list[4], (SEQS, CONV - 1, INNER), 1.0, 6.0, ((0, 8), (2, 4)))
    conv_b = noise(key_list[5], (SEQS, CONV - 1, G * N), 1.0, 6.0, ((0, 8), (2, 4)))
    conv_c = noise(key_list[6], (SEQS, CONV - 1, G * N), 1.0, 6.0, ((0, 8), (2, 4)))
    path_x = noise(key_list[7], (SEQS, P_SIZE, INNER), 1.0, 6.0, ((0, 8), (2, 4)))
    path_b = noise(key_list[8], (SEQS, P_SIZE, G * N), 1.0, 6.0, ((0, 8), (2, 4)))
    path_c = noise(key_list[9], (SEQS, P_SIZE, G * N), 1.0, 6.0, ((0, 8), (2, 4)))
    path_dt = noise(key_list[10], (SEQS, P_SIZE, H), 1.0, 6.0, ((0, 8), (2, 4)))
    gain_in = jnp.clip(1.0 + 0.18 * jax.random.normal(key_list[11], (D,), jnp.float32), 0.1, 1.9)
    w_x = noise(key_list[12], (D, INNER), D ** -0.5, 0.09375, ((0, 8), (1, 4)))
    w_z = noise(key_list[13], (D, INNER), D ** -0.5, 0.09375, ((0, 8), (1, 4)))
    w_b = noise(key_list[14], (D, G * N), D ** -0.5, 0.09375, ((0, 8), (1, 4)))
    w_c = noise(key_list[15], (D, G * N), D ** -0.5, 0.09375, ((0, 8), (1, 4)))
    w_dt = noise(key_list[16], (D, H), D ** -0.5, 0.09375)
    dt_bias = jnp.clip(-2.0 + 3.0 * jax.random.uniform(key_list[17], (H,), jnp.float32) ** block_scale(key_list[17], (H,), ((0, 4),), -0.2, 0.2), -2.0, 1.0)
    a_log = jnp.clip(-3.0 + 4.5 * jax.random.uniform(key_list[18], (H,), jnp.float32) ** block_scale(key_list[18], (H,), ((0, 4),), -0.2, 0.2), -3.0, 1.5)
    d_skip = jnp.clip(0.5 + 1.0 * jax.random.uniform(key_list[19], (H,), jnp.float32) ** block_scale(key_list[19], (H,), ((0, 4),), -0.2, 0.2), 0.5, 1.5)
    conv_wx = noise(key_list[20], (CONV, INNER), 0.5, 3.0, ((1, 4),))
    conv_wb = noise(key_list[21], (CONV, G * N), 0.5, 3.0, ((1, 4),))
    conv_wc = noise(key_list[22], (CONV, G * N), 0.5, 3.0, ((1, 4),))
    gain_out = jnp.clip(1.0 + 0.18 * jax.random.normal(key_list[23], (INNER,), jnp.float32), 0.1, 1.9)
    w_out = noise(key_list[24], (INNER, D), INNER ** -0.5, 0.09375, ((0, 4), (1, 8)))
    return dict(tokens=tokens, parents=parents, accepted=accepted, state=state, conv_x=conv_x, conv_b=conv_b, conv_c=conv_c, path_x=path_x, path_b=path_b, path_c=path_c, path_dt=path_dt, gain_in=gain_in, w_x=w_x, w_z=w_z, w_b=w_b, w_c=w_c, w_dt=w_dt, dt_bias=dt_bias, a_log=a_log, d_skip=d_skip, conv_wx=conv_wx, conv_wb=conv_wb, conv_wc=conv_wc, gain_out=gain_out, w_out=w_out)


EPS = 1e-06
HIGH = lax.Precision.HIGHEST

def conv_window(history, taps, amount):
    values = history.astype(jnp.float32)
    weights = taps.astype(jnp.float32)
    summed = weights[0] * values[:, 0:amount, :]
    for distance in range(1, weights.shape[0]):
        summed = summed + weights[distance] * values[:, distance:distance + amount, :]
    return jax.nn.silu(summed)

def commit_rows(history, accepted, keep):
    picked = accepted[:, None].astype(jnp.int32) + jnp.arange(keep, dtype=jnp.int32)[None, :]
    select = (picked[:, :, None] == jnp.arange(history.shape[1], dtype=jnp.int32)[None, None, :]).astype(jnp.float32)
    return jnp.einsum('skl,slc->skc', select, history.astype(jnp.float32), precision=HIGH).astype(jnp.bfloat16)

def replay_state(state, history_x, history_b, path_dt, conv_wx, conv_wb, accepted, rate_bias, a_rate, per_group):
    seq_count, heads, head_dim, state_dim = state.shape
    path_len = path_dt.shape[1]
    path_xs = conv_window(history_x, conv_wx, path_len).reshape(seq_count, path_len, heads, head_dim)
    path_bs = conv_window(history_b, conv_wb, path_len).reshape(seq_count, path_len, heads // per_group, state_dim)
    path_bh = jnp.repeat(path_bs, per_group, axis=2)
    path_step = jax.nn.softplus(path_dt.astype(jnp.float32) + rate_bias)
    is_live = (jnp.arange(path_len, dtype=jnp.int32)[None, :] < accepted[:, None].astype(jnp.int32)).astype(jnp.float32)[:, :, None]
    log_decay = path_step * a_rate * is_live
    overall = lax.optimization_barrier(jnp.sum(log_decay, axis=1))
    tail_sum = overall[:, None, :] - jnp.cumsum(log_decay, axis=1)
    weights = is_live * jnp.exp(tail_sum) * path_step
    grown = jnp.einsum('sjh,sjhp,sjhn->shpn', weights, path_xs, path_bh, precision=HIGH)
    return jnp.exp(overall)[:, :, None, None] * state + grown

def tree_links(parents, keep):
    seq_count, prop_count = parents.shape
    front = jnp.broadcast_to(jnp.arange(-1, keep - 1, dtype=jnp.int32)[None, :], (seq_count, keep))
    parent_ids = jnp.concatenate([front, parents.astype(jnp.int32) + keep], axis=1)
    nodes = keep + prop_count
    links = (parent_ids[:, :, None] == jnp.arange(nodes, dtype=jnp.int32)[None, None, :]).astype(jnp.float32)
    identity = jnp.eye(prop_count, dtype=jnp.float32)[None, :, :]
    ancestry = identity + links[:, keep:, keep:]
    for turn in range(prop_count.bit_length()):
        ancestry = jnp.minimum(jnp.einsum('sij,sjk->sik', ancestry, ancestry, precision=HIGH), 1.0)
    return (links, ancestry)

def tree_conv(buffer, rows, taps, links, keep):
    values = jnp.concatenate([buffer, rows], axis=1).astype(jnp.float32)
    weights = taps.astype(jnp.float32)
    last_tap = weights.shape[0] - 1
    summed = weights[last_tap] * values
    reached = values
    for distance in range(1, last_tap + 1):
        reached = jnp.einsum('sij,sjc->sic', links, reached, precision=HIGH)
        summed = summed + weights[last_tap - distance] * reached
    return jax.nn.silu(summed[:, keep:, :])

def tree_mix(state, post_x, post_b, post_c, rate_rows, z_rows, ancestry, rate_bias, a_rate, d_skip, gain_out, per_group):
    seq_count, prop_count, _ = post_x.shape
    heads, head_dim, state_dim = (state.shape[1], state.shape[2], state.shape[3])
    groups = heads // per_group
    x_heads = post_x.reshape(seq_count, prop_count, heads, head_dim)
    b_groups = post_b.reshape(seq_count, prop_count, groups, state_dim)
    c_groups = post_c.reshape(seq_count, prop_count, groups, state_dim)
    step_size = jax.nn.softplus(rate_rows.astype(jnp.float32) + rate_bias)
    path_decay = jnp.einsum('sij,sjh->sih', ancestry, step_size * a_rate, precision=HIGH)
    c_heads = jnp.repeat(c_groups, per_group, axis=2)
    carried = jnp.einsum('sihn,shpn->sihp', c_heads, state, precision=HIGH) * jnp.exp(path_decay)[:, :, :, None]
    scores = jnp.einsum('sign,sjgn->sgij', c_groups, b_groups, precision=HIGH)
    scores = jnp.repeat(scores, per_group, axis=1)
    decay_t = jnp.transpose(path_decay, (0, 2, 1))
    decay_gap = decay_t[:, :, :, None] - decay_t[:, :, None, :]
    is_live = ancestry[:, None, :, :] > 0.5
    mixing = jnp.where(is_live, jnp.exp(jnp.where(is_live, decay_gap, 0.0)), 0.0)
    mixing = mixing * jnp.transpose(step_size, (0, 2, 1))[:, :, None, :]
    within = jnp.einsum('shij,sjhp->sihp', scores * mixing, x_heads, precision=HIGH)
    heads_out = carried + within + d_skip[None, None, :, None] * x_heads
    heads_out = heads_out.reshape(seq_count, prop_count, heads * head_dim) * jax.nn.silu(z_rows.astype(jnp.float32))
    grouped = heads_out.reshape(seq_count, prop_count, groups, per_group * head_dim)
    grouped = grouped * lax.rsqrt(lax.optimization_barrier(jnp.mean(grouped * grouped, axis=-1, keepdims=True)) + EPS)
    return (grouped.reshape(seq_count, prop_count, heads * head_dim) * gain_out).astype(jnp.bfloat16)

def reference(tokens, parents, accepted, state, conv_x, conv_b, conv_c, path_x, path_b, path_c, path_dt, gain_in, w_x, w_z, w_b, w_c, w_dt, dt_bias, a_log, d_skip, conv_wx, conv_wb, conv_wc, gain_out, w_out):
    seq_count, prop_count, width = tokens.shape
    keep = conv_wx.shape[0] - 1
    flat_rows = tokens.reshape(-1, width).astype(jnp.float32)
    row_scale = lax.rsqrt(lax.optimization_barrier(jnp.sum(flat_rows * flat_rows, axis=1)) / width + EPS)[:, None]
    scaled = (flat_rows * gain_in).astype(jnp.bfloat16)

    def project(weight):
        product = jnp.dot(scaled, weight, preferred_element_type=jnp.float32) * row_scale
        return product.astype(jnp.bfloat16).reshape(seq_count, prop_count, -1)
    x_rows = project(w_x)
    z_rows = project(w_z)
    b_rows = project(w_b)
    c_rows = project(w_c)
    rate_rows = project(w_dt)
    a_rate = -jnp.exp(a_log)
    history_x = jnp.concatenate([conv_x, path_x], axis=1)
    history_b = jnp.concatenate([conv_b, path_b], axis=1)
    history_c = jnp.concatenate([conv_c, path_c], axis=1)
    new_state = replay_state(state, history_x, history_b, path_dt, conv_wx, conv_wb, accepted, dt_bias, a_rate, HPG)
    links, ancestry = tree_links(parents, keep)
    post_x = tree_conv(commit_rows(history_x, accepted, keep), x_rows, conv_wx, links, keep)
    post_b = tree_conv(commit_rows(history_b, accepted, keep), b_rows, conv_wb, links, keep)
    post_c = tree_conv(commit_rows(history_c, accepted, keep), c_rows, conv_wc, links, keep)
    gated = tree_mix(new_state, post_x, post_b, post_c, rate_rows, z_rows, ancestry, dt_bias, a_rate, d_skip, gain_out, HPG)
    block = gated.shape[2] // N_TP
    gated_flat = gated.reshape(-1, gated.shape[2])
    running = jnp.zeros((gated_flat.shape[0], width), jnp.float32)
    for index in range(N_TP):
        term = jnp.dot(gated_flat[:, index * block:(index + 1) * block], w_out[index * block:(index + 1) * block, :], preferred_element_type=jnp.float32)
        rounded = lax.optimization_barrier(term.astype(jnp.bfloat16))
        running = running + rounded.astype(jnp.float32)
    mixed = running.astype(jnp.bfloat16).reshape(seq_count, prop_count, width)
    return (mixed, new_state)
```

```python
import functools

import jax
import jax.numpy as jnp
from jax import lax
from jax.experimental import pallas as pl
from jax.experimental.pallas import tpu as pltpu
from jax.sharding import PartitionSpec as P

HPG = 4


EPS = 1e-06
HIGH = lax.Precision.HIGHEST
LANES = 128


def log2(count):
    return count.bit_length() - 1


def flipped_bits(position, order):
    value = 0
    for place, bit in enumerate(order):
        value |= ((position >> (len(order) - 1 - place)) & 1) << bit
    return value


def scale_kernel(orders, me_ref, tokens_ref, gain_ref, *out_refs):
    props, blocks, seqs, width = tokens_ref.shape
    me = me_ref[0]
    squares_ref = out_refs[-1]
    for which, order in enumerate(orders):
        for position in range(blocks):
            rows = tokens_ref[:, me ^ flipped_bits(position, order)].astype(jnp.float32)
            rows = rows.reshape(props * seqs, width)
            out_refs[which][position] = (rows * gain_ref[...]).astype(jnp.bfloat16)
            if which == len(orders) - 1:
                squares_ref[position] = jnp.sum(rows * rows, axis=1, keepdims=True)


def scale_rows(orders, me, tokens, gain):
    props, blocks, seqs, width = tokens.shape
    shape = (blocks, props * seqs, width)
    return pl.pallas_call(
        functools.partial(scale_kernel, orders),
        out_shape=[jax.ShapeDtypeStruct(shape, jnp.bfloat16) for _ in orders]
        + [jax.ShapeDtypeStruct((blocks, props * seqs, 1), jnp.float32)],
        in_specs=[
            pl.BlockSpec(memory_space=pltpu.SMEM),
            pl.BlockSpec(memory_space=pltpu.VMEM),
            pl.BlockSpec(memory_space=pltpu.VMEM),
        ],
        out_specs=[pl.BlockSpec(memory_space=pltpu.VMEM) for _ in range(len(orders) + 1)],
        name="scale_rows",
    )(me.reshape(1), tokens, gain)


def swap_bit(array, bit, blocks):
    return lax.ppermute(array, "kv", [(i, i ^ (1 << bit)) for i in range(blocks)])


def halving(keep, received, order, blocks):
    for bit in order:
        half = keep.shape[0] // 2
        send = keep[half:].astype(jnp.float32) + received[half:].astype(jnp.float32)
        arriving = swap_bit(send.astype(jnp.bfloat16), bit, blocks)
        keep = keep[:half].astype(jnp.float32) + received[:half].astype(jnp.float32)
        received = arriving
    return keep.astype(jnp.float32) + received.astype(jnp.float32)


def project(scaled, weight):
    return jnp.dot(scaled, weight, preferred_element_type=jnp.float32)


def conv_window(history, taps, amount):
    values = history.astype(jnp.float32)
    weights = taps.astype(jnp.float32)
    summed = weights[0] * values[:, 0:amount, :]
    for distance in range(1, weights.shape[0]):
        summed = summed + weights[distance] * values[:, distance : distance + amount, :]
    return jax.nn.silu(summed)


def commit_rows(history, accepted, keep):
    picked = accepted[:, None] + jnp.arange(keep, dtype=jnp.int32)[None, :]
    select = (
        picked[:, :, None] == jnp.arange(history.shape[1], dtype=jnp.int32)[None, None, :]
    ).astype(jnp.float32)
    return jnp.einsum("skl,slc->skc", select, history.astype(jnp.float32), precision=HIGH).astype(
        jnp.bfloat16
    )


def replay_state(
    state, history_x, history_b, path_dt, conv_wx, conv_wb, accepted, rate_bias, a_rate, per_group
):
    seq_count, heads, head_dim, state_dim = state.shape
    path_len = path_dt.shape[1]
    path_xs = conv_window(history_x, conv_wx, path_len).reshape(
        seq_count, path_len, heads, head_dim
    )
    path_bs = conv_window(history_b, conv_wb, path_len).reshape(
        seq_count, path_len, heads // per_group, state_dim
    )
    path_bh = jnp.repeat(path_bs, per_group, axis=2)
    path_step = jax.nn.softplus(path_dt.astype(jnp.float32) + rate_bias)
    is_live = (jnp.arange(path_len, dtype=jnp.int32)[None, :] < accepted[:, None]).astype(
        jnp.float32
    )[:, :, None]
    log_decay = path_step * a_rate * is_live
    overall = jnp.sum(log_decay, axis=1)
    tail_sum = overall[:, None, :] - jnp.cumsum(log_decay, axis=1)
    weights = is_live * jnp.exp(tail_sum) * path_step
    grown = jnp.einsum("sjh,sjhp,sjhn->shpn", weights, path_xs, path_bh, precision=HIGH)
    return jnp.exp(overall)[:, :, None, None] * state + grown


def tree_links(parents, keep):
    seq_count, prop_count = parents.shape
    front = jnp.broadcast_to(jnp.arange(-1, keep - 1, dtype=jnp.int32)[None, :], (seq_count, keep))
    parent_ids = jnp.concatenate([front, parents + keep], axis=1)
    nodes = keep + prop_count
    links = (parent_ids[:, :, None] == jnp.arange(nodes, dtype=jnp.int32)[None, None, :]).astype(
        jnp.float32
    )
    identity = jnp.eye(prop_count, dtype=jnp.float32)[None, :, :]
    ancestry = identity + links[:, keep:, keep:]
    for turn in range(prop_count.bit_length()):
        ancestry = jnp.minimum(jnp.einsum("sij,sjk->sik", ancestry, ancestry, precision=HIGH), 1.0)
    return (links, ancestry)


def tree_conv(buffer, rows, taps, links, keep):
    values = jnp.concatenate([buffer, rows], axis=1).astype(jnp.float32)
    weights = taps.astype(jnp.float32)
    last_tap = weights.shape[0] - 1
    summed = weights[last_tap] * values
    reached = values
    for distance in range(1, last_tap + 1):
        reached = jnp.einsum("sij,sjc->sic", links, reached, precision=HIGH)
        summed = summed + weights[last_tap - distance] * reached
    return jax.nn.silu(summed[:, keep:, :])


def tree_mix(
    state,
    post_x,
    post_b,
    post_c,
    rate_rows,
    z_rows,
    ancestry,
    rate_bias,
    a_rate,
    d_skip,
    gain_out,
    per_group,
):
    seq_count, prop_count, _ = post_x.shape
    heads, head_dim, state_dim = (state.shape[1], state.shape[2], state.shape[3])
    groups = heads // per_group
    x_heads = post_x.reshape(seq_count, prop_count, heads, head_dim)
    b_groups = post_b.reshape(seq_count, prop_count, groups, state_dim)
    c_groups = post_c.reshape(seq_count, prop_count, groups, state_dim)
    step_size = jax.nn.softplus(rate_rows.astype(jnp.float32) + rate_bias)
    path_decay = jnp.einsum("sij,sjh->sih", ancestry, step_size * a_rate, precision=HIGH)
    c_heads = jnp.repeat(c_groups, per_group, axis=2)
    carried = (
        jnp.einsum("sihn,shpn->sihp", c_heads, state, precision=HIGH)
        * jnp.exp(path_decay)[:, :, :, None]
    )
    scores = jnp.einsum("sign,sjgn->sgij", c_groups, b_groups, precision=HIGH)
    scores = jnp.repeat(scores, per_group, axis=1)
    decay_t = jnp.transpose(path_decay, (0, 2, 1))
    decay_gap = decay_t[:, :, :, None] - decay_t[:, :, None, :]
    is_live = ancestry[:, None, :, :] > 0.5
    mixing = jnp.where(is_live, jnp.exp(jnp.where(is_live, decay_gap, 0.0)), 0.0)
    mixing = mixing * jnp.transpose(step_size, (0, 2, 1))[:, :, None, :]
    within = jnp.einsum("shij,sjhp->sihp", scores * mixing, x_heads, precision=HIGH)
    heads_out = carried + within + d_skip[None, None, :, None] * x_heads
    heads_out = heads_out.reshape(seq_count, prop_count, heads * head_dim) * jax.nn.silu(
        z_rows.astype(jnp.float32)
    )
    grouped = heads_out.reshape(seq_count, prop_count, groups, per_group * head_dim)
    grouped = grouped * lax.rsqrt(jnp.mean(grouped * grouped, axis=-1, keepdims=True) + EPS)
    return (grouped.reshape(seq_count, prop_count, heads * head_dim) * gain_out).astype(
        jnp.bfloat16
    )


def shards(
    kv_count,
    tp_count,
    tokens,
    parents,
    accepted,
    state,
    conv_x,
    conv_b,
    conv_c,
    path_x,
    path_b,
    path_c,
    path_dt,
    gain_in,
    w_x,
    w_z,
    w_b,
    w_c,
    w_dt,
    dt_bias,
    a_log,
    d_skip,
    conv_wx,
    conv_wb,
    conv_wc,
    gain_out,
    w_out,
):
    seq_local = state.shape[0]
    proposals = parents.shape[1]
    heads_local = dt_bias.shape[0]
    inner_local = w_x.shape[1]
    group_cols = w_b.shape[1]
    width = gain_in.shape[0]
    keep = conv_wx.shape[0] - 1
    tp_index = lax.axis_index("tp")
    kv_index = lax.axis_index("kv")
    slab_width = tokens.shape[2]
    rows_local = seq_local * proposals
    z_count = tp_count
    x_count = kv_count // z_count
    x_bits = list(range(log2(x_count)))
    z_bits = list(range(log2(x_count), log2(kv_count)))
    x_first = x_bits + z_bits
    z_first = z_bits + x_bits
    x_place = kv_index % x_count
    z_place = kv_index // x_count

    gain_part = lax.dynamic_slice_in_dim(gain_in, kv_index * slab_width, slab_width)
    tokens_q = tokens.transpose(1, 0, 2).reshape(proposals, kv_count, seq_local, slab_width)
    scaled_x, scaled_z, squares = scale_rows(
        (x_first, z_first), kv_index, tokens_q, gain_part[None, :]
    )
    half_rows = rows_local * kv_count // 2
    scaled_x = scaled_x.reshape(2, half_rows, slab_width)
    scaled_z = scaled_z.reshape(2, half_rows, slab_width)
    squares = squares.reshape(2, half_rows, 1)
    w_rate = lax.dynamic_slice(
        w_dt, (kv_index * slab_width, tp_index * heads_local), (slab_width, heads_local)
    )
    w_bcr = jnp.concatenate(
        [w_b, w_c, w_rate, jnp.zeros((slab_width, LANES - heads_local), w_b.dtype)], axis=1
    )
    square_col = (
        jnp.arange(2 * group_cols + LANES, dtype=jnp.int32)[None, :]
        == 2 * group_cols + heads_local
    )

    def project_bcr(part):
        return (
            project(scaled_z[part], w_bcr) + jnp.where(square_col, squares[part], 0.0)
        ).astype(jnp.bfloat16)

    def summed(scaled, weight, order):
        got = swap_bit(project(scaled[1], weight).astype(jnp.bfloat16), order[0], kv_count)
        own = project(scaled[0], weight).astype(jnp.bfloat16)
        return halving(own, got, order[1:], kv_count)

    got_bcr = swap_bit(project_bcr(1), z_first[0], kv_count)
    x_sum = summed(scaled_x, w_x, x_first)
    z_sum = summed(scaled_x, w_z, x_first)
    bcr_sum = halving(project_bcr(0), got_bcr, z_first[1:], kv_count)

    w_pieces = [w_out]
    for bit in x_bits:
        w_pieces = w_pieces + [swap_bit(piece, bit, kv_count) for piece in w_pieces]
    for bit in x_bits:
        flip = ((kv_index >> bit) & 1) == 1
        w_pieces = [
            jnp.where(flip, w_pieces[place ^ (1 << bit)], w_pieces[place])
            for place in range(x_count)
        ]
    w_block = jnp.concatenate(w_pieces, axis=1)

    row_scale = lax.rsqrt(
        bcr_sum[:, 2 * group_cols + heads_local : 2 * group_cols + heads_local + 1] / width + EPS
    )

    def rows_of(values):
        values = (values * row_scale).astype(jnp.bfloat16)
        return values.reshape(proposals, seq_local, -1).transpose(1, 0, 2)

    x_rows = rows_of(x_sum)
    z_rows = rows_of(z_sum)
    b_rows = rows_of(bcr_sum[:, :group_cols])
    c_rows = rows_of(bcr_sum[:, group_cols : 2 * group_cols])
    rate_rows = rows_of(bcr_sum[:, 2 * group_cols : 2 * group_cols + heads_local])
    a_rate = -jnp.exp(a_log)
    history_x = jnp.concatenate([conv_x, path_x], axis=1)
    history_b = jnp.concatenate([conv_b, path_b], axis=1)
    history_c = jnp.concatenate([conv_c, path_c], axis=1)
    new_state = replay_state(
        state, history_x, history_b, path_dt, conv_wx, conv_wb, accepted, dt_bias, a_rate, HPG
    )
    links, ancestry = tree_links(parents, keep)
    post_x = tree_conv(commit_rows(history_x, accepted, keep), x_rows, conv_wx, links, keep)
    post_b = tree_conv(commit_rows(history_b, accepted, keep), b_rows, conv_wb, links, keep)
    post_c = tree_conv(commit_rows(history_c, accepted, keep), c_rows, conv_wc, links, keep)
    gated = tree_mix(
        new_state,
        post_x,
        post_b,
        post_c,
        rate_rows,
        z_rows,
        ancestry,
        dt_bias,
        a_rate,
        d_skip,
        gain_out,
        HPG,
    )
    gated_flat = gated.transpose(1, 0, 2).reshape(-1, inner_local)
    pieces = {0: gated_flat}
    for bit in z_bits[::-1]:
        for place in list(pieces):
            pieces[place | (1 << (bit - len(x_bits)))] = swap_bit(pieces[place], bit, kv_count)
    terms = [
        project(pieces[place], w_block).astype(jnp.bfloat16) for place in range(z_count)
    ]
    core_flip = ((tp_index ^ z_place) & 1) == 1
    sent = []
    kept = []
    for place in range(0, z_count, 2):
        sent.append(jnp.where(core_flip, terms[place], terms[place + 1]))
        kept.append(jnp.where(core_flip, terms[place + 1], terms[place]))
    swapped = lax.ppermute(
        jnp.concatenate(sent, axis=0), "tp", [(i, i ^ 1) for i in range(tp_count)]
    )
    half = z_count // 2
    paired = (
        jnp.concatenate(kept, axis=0).astype(jnp.float32) + swapped.astype(jnp.float32)
    ).astype(jnp.bfloat16).reshape(half, rows_local, -1)
    total = 0.0
    for shift in range(half):
        block = (tp_index >> 1) ^ (z_place >> 1) ^ shift
        links_out = []
        for z in range(z_count):
            for x in range(x_count):
                for t in range(tp_count):
                    z_to = (((t >> 1) ^ shift) << 1) | (t & 1)
                    links_out.append(
                        ((z * x_count + x) * tp_count + t, (z_to * x_count + x) * tp_count + z)
                    )
        piece = lax.dynamic_index_in_dim(paired, block, 0, keepdims=False)
        total = total + lax.ppermute(piece, ("kv", "tp"), links_out).astype(jnp.float32)
    mixed = total.astype(jnp.bfloat16).reshape(proposals, seq_local, -1).transpose(1, 0, 2)
    return (mixed, new_state)


def solution(mesh):
    return jax.shard_map(
        functools.partial(shards, mesh.shape["kv"], mesh.shape["tp"]),
        mesh=mesh,
        in_specs=(
            P(None, None, "kv"),
            P("kv", None),
            P("kv"),
            P("kv", "tp", None, None),
            P("kv", None, "tp"),
            P("kv", None, "tp"),
            P("kv", None, "tp"),
            P("kv", None, "tp"),
            P("kv", None, "tp"),
            P("kv", None, "tp"),
            P("kv", None, "tp"),
            P(),
            P("kv", "tp"),
            P("kv", "tp"),
            P("kv", "tp"),
            P("kv", "tp"),
            P(),
            P("tp"),
            P("tp"),
            P("tp"),
            P(None, "tp"),
            P(None, "tp"),
            P(None, "tp"),
            P("tp"),
            P("tp", "kv"),
        ),
        out_specs=(P("kv", None, "tp"), P("kv", "tp", None, None)),
        check_vma=False,
    )
```

```python
import functools

import jax
import jax.numpy as jnp
from jax import lax
from jax.experimental import pallas as pl
from jax.experimental.pallas import tpu as pltpu
from jax.sharding import PartitionSpec as P


HPG = 4
EPS = 1e-06
LANES = 128
CHUNK = 256
VMEM = pltpu.VMEM
F32 = jnp.float32
BF16 = jnp.bfloat16
NT = (((1,), (1,)), ((), ()))


def log2(count):
    return count.bit_length() - 1


def flipped_bits(position, order):
    value = 0
    for place, bit in enumerate(order):
        value |= ((position >> (len(order) - 1 - place)) & 1) << bit
    return value


def whole(count):
    return [pl.BlockSpec(memory_space=VMEM) for _ in range(count)]


def cost(microseconds):
    return pl.CostEstimate(
        flops=int(microseconds * 4e6), bytes_accessed=1024, transcendentals=0
    )


def dot(left, right):
    return jnp.dot(left, right, preferred_element_type=F32)


def dot_nt(left, right):
    return lax.dot_general(left, right, NT, preferred_element_type=F32)


def silu(values):
    return values / (1.0 + jnp.exp(-values))


def softplus(values):
    return jnp.maximum(values, 0.0) + jnp.log1p(jnp.exp(-jnp.abs(values)))


def project_kernel(differences, with_rate, tp_count, tokens_ref, gain_ref, *refs):
    props, _, seqs, width = tokens_ref.shape
    me = lax.axis_index("kv")
    rows_local = props * seqs
    if with_rate:
        w_dt_ref, *w_refs, out_ref, scaled_ref, squares_ref = refs
    else:
        *w_refs, out_ref, scaled_ref = refs
    slab_start = pl.multiple_of(me * width, LANES)
    gain = gain_ref[:, pl.ds(slab_start, width)]
    for position, difference in enumerate(differences):
        rows = tokens_ref[:, me ^ difference].astype(F32).reshape(rows_local, width)
        span = slice(position * rows_local, (position + 1) * rows_local)
        scaled_ref[span] = (rows * gain).astype(BF16)
        if with_rate:
            squares_ref[span] = jnp.sum(rows * rows, axis=1, keepdims=True)
    start = 0
    for w_ref in w_refs:
        for lower in range(0, w_ref.shape[1], CHUNK):
            upper = min(lower + CHUNK, w_ref.shape[1])
            out_ref[:, start + lower : start + upper] = dot(
                scaled_ref[...], w_ref[:, lower:upper]
            ).astype(BF16)
        start += w_ref.shape[1]
    if with_rate:
        heads = w_dt_ref.shape[0]
        local = heads // tp_count
        first = lax.axis_index("tp") * local
        row = lax.broadcasted_iota(jnp.int32, (LANES, heads), 0)
        column = lax.broadcasted_iota(jnp.int32, (LANES, heads), 1)
        pick = jnp.where((row < local) & (column == row + first), 1.0, 0.0).astype(BF16)
        slab = w_dt_ref[:, pl.ds(slab_start, width)]
        w_rate = dot(pick, slab).astype(BF16)
        lane = lax.broadcasted_iota(jnp.int32, (1, LANES), 1)
        rate = dot_nt(scaled_ref[...], w_rate)
        out_ref[:, start : start + LANES] = jnp.where(
            lane == local, squares_ref[...], rate
        ).astype(BF16)


def project(differences, tokens, tp_count, gain, weights, w_dt=None):
    props, _, seqs, width = tokens.shape
    rows = len(differences) * props * seqs
    columns = sum(weight.shape[1] for weight in weights)
    scratch = [pltpu.VMEM((rows, width), BF16)]
    operands = [tokens, gain]
    if w_dt is not None:
        columns += LANES
        scratch.append(pltpu.VMEM((rows, 1), F32))
        operands.append(w_dt)
    operands += list(weights)
    return pl.pallas_call(
        functools.partial(project_kernel, tuple(differences), w_dt is not None, tp_count),
        out_shape=jax.ShapeDtypeStruct((rows, columns), BF16),
        in_specs=whole(len(operands)),
        out_specs=pl.BlockSpec(memory_space=VMEM),
        scratch_shapes=scratch,
        cost_estimate=cost(2),
        name="project",
    )(*operands)


def window(conv_ref, path_ref, taps_ref, seqs):
    history = jnp.concatenate([conv_ref[...].astype(F32), path_ref[...].astype(F32)], axis=0)
    count = path_ref.shape[0]
    taps = taps_ref[...].astype(F32)
    total = taps[0:1] * history[0:count]
    for distance in range(1, taps.shape[0]):
        total = total + taps[distance : distance + 1] * history[
            distance * seqs : distance * seqs + count
        ]
    return silu(total)


def split(values):
    high = values.astype(BF16).astype(F32)
    return high, values - high


def state_kernel(
    accepted_ref,
    path_dt_ref,
    bias_ref,
    a_log_ref,
    conv_x_ref,
    path_x_ref,
    taps_x_ref,
    conv_b_ref,
    path_b_ref,
    taps_b_ref,
    state_ref,
    out_ref,
    half_ref,
    left_ref,
    right_ref,
    decay_ref,
):
    _, heads, head_dim, state_dim = state_ref.shape
    seqs = accepted_ref.shape[0]
    sequence = pl.program_id(0)
    count = path_x_ref.shape[0]
    group_width = HPG * head_dim

    @pl.when(sequence == 0)
    def _():
        lane = lax.broadcasted_iota(jnp.int32, (heads, heads * head_dim), 1)
        row = lax.broadcasted_iota(jnp.int32, (heads, heads * head_dim), 0)
        spread = jnp.where(lane // head_dim == row, 1.0, 0.0).astype(BF16)
        accepted = accepted_ref[...]
        a_rate = -jnp.exp(a_log_ref[...])
        steps = softplus(path_dt_ref[...].astype(F32) + bias_ref[...])
        weights = []
        overall = jnp.zeros((seqs, heads), F32)
        for position in range(count // seqs - 1, -1, -1):
            step = steps[position * seqs : (position + 1) * seqs]
            live = jnp.where(position < accepted, 1.0, 0.0)
            weights.append(live * jnp.exp(overall) * step)
            overall = overall + step * a_rate * live
        decay_ref[...] = jnp.exp(overall)
        high, low = split(jnp.concatenate(weights[::-1], axis=0))
        weights = dot(high.astype(BF16), spread) + dot(low.astype(BF16), spread)
        grown = weights * window(conv_x_ref, path_x_ref, taps_x_ref, seqs)
        empty = jnp.zeros((LANES - 2 * count, grown.shape[1]), F32)
        turned = jnp.concatenate([grown, grown, empty], axis=0).T
        high, low = split(turned)
        left_ref[:, :LANES] = high.astype(BF16)
        left_ref[:, LANES:] = low.astype(BF16)
        rows_b = window(conv_b_ref, path_b_ref, taps_b_ref, seqs)
        high, low = split(rows_b)
        right_ref[...] = jnp.zeros_like(right_ref)
        right_ref[0:count] = high
        right_ref[count : 2 * count] = low
        right_ref[LANES : LANES + count] = high

    row = lax.broadcasted_iota(jnp.int32, (2 * LANES, 1), 0)
    mine = jnp.where(lax.rem(row, seqs) == sequence, 1.0, 0.0)
    right = (right_ref[...] * mine).astype(BF16)
    decay = decay_ref[pl.ds(sequence, 1), :]
    for group in range(heads // HPG):
        grown = dot(
            left_ref[group * group_width : (group + 1) * group_width],
            right[:, group * state_dim : (group + 1) * state_dim],
        )
        for head in range(HPG):
            index = group * HPG + head
            value = decay[:, index : index + 1] * state_ref[0, index] + grown[
                head * head_dim : (head + 1) * head_dim
            ]
            out_ref[0, index] = value
            half_ref[0, index] = value.astype(BF16)


def replay_state(accepted, path_dt, bias, a_log, conv_x, path_x, taps_x, conv_b, path_b, taps_b, state):
    seqs, heads, head_dim, state_dim = state.shape
    block = pl.BlockSpec((1, heads, head_dim, state_dim), lambda s: (s, 0, 0, 0))

    def full(array):
        return pl.BlockSpec(array.shape, lambda s: (0,) * array.ndim)

    small = [accepted, path_dt, bias, a_log, conv_x, path_x, taps_x, conv_b, path_b, taps_b]
    return pl.pallas_call(
        state_kernel,
        grid=(seqs,),
        out_shape=[
            jax.ShapeDtypeStruct(state.shape, F32),
            jax.ShapeDtypeStruct(state.shape, BF16),
        ],
        in_specs=[full(a) for a in small] + [block],
        out_specs=[block, block],
        scratch_shapes=[
            pltpu.VMEM((heads * head_dim, 2 * LANES), BF16),
            pltpu.VMEM((2 * LANES, path_b.shape[1]), F32),
            pltpu.VMEM((seqs, heads), F32),
        ],
        cost_estimate=cost(8),
        name="replay_state",
    )(*small, state)


def tree_kernel(parents_ref, accepted_ref, *refs):
    *inputs, links_ref, ancestry_ref, before_ref = refs
    seqs, props = parents_ref.shape
    nodes = seqs * props
    parents = parents_ref[...]
    parent = jnp.concatenate([parents[:, place : place + 1] for place in range(props)], axis=0)
    accepted = jnp.concatenate([accepted_ref[...]] * props, axis=0)
    row = lax.broadcasted_iota(jnp.int32, (nodes, nodes), 0)
    column = lax.broadcasted_iota(jnp.int32, (nodes, nodes), 1)
    own = lax.rem(lax.broadcasted_iota(jnp.int32, (nodes, 1), 0), seqs)
    target = jnp.where(parent >= 0, parent * seqs + own, -1)
    link = jnp.where(column == target, 1.0, 0.0)
    ancestry = link + jnp.where(row == column, 1.0, 0.0)
    link = link.astype(BF16)
    reach = link
    taps_count = inputs[2].shape[0]
    for distance in range(1, taps_count):
        links_ref[(distance - 1) * nodes : distance * nodes] = reach
        reach = dot(reach, link).astype(BF16)
    for _ in range(props.bit_length()):
        half = ancestry.astype(BF16)
        ancestry = jnp.minimum(dot(half, half), 1.0)
    ancestry_ref[...] = ancestry
    depth = jnp.sum(ancestry, axis=1, keepdims=True).astype(jnp.int32) - 1
    last = taps_count - 1

    def chosen(first, rows, distance):
        lane = lax.broadcasted_iota(jnp.int32, (nodes, rows), 1)
        wanted = accepted + last - distance + depth
        hit = (lane // seqs + first == wanted) & (lax.rem(lane, seqs) == own)
        return jnp.where(hit & (depth < distance), 1.0, 0.0).astype(BF16)

    conv_rows = inputs[0].shape[0]
    path_rows = inputs[1].shape[0]
    picks = [
        (chosen(0, conv_rows, d), chosen(conv_rows // seqs, path_rows, d))
        for d in range(1, taps_count)
    ]
    start = 0
    for which in range(0, len(inputs), 3):
        conv_ref, path_ref, taps_ref = inputs[which : which + 3]
        taps = taps_ref[...].astype(F32)
        total = 0.0
        for distance in range(1, taps_count):
            early, late = picks[distance - 1]
            found = dot(early, conv_ref[...]) + dot(late, path_ref[...])
            total = total + taps[last - distance : last - distance + 1] * found
        before_ref[:, start : start + conv_ref.shape[1]] = total
        start += conv_ref.shape[1]


def tree(parents, accepted, streams):
    nodes = parents.shape[0] * parents.shape[1]
    inputs = [array for stream in streams for array in stream]
    width = sum(stream[0].shape[1] for stream in streams)
    taps_count = streams[0][2].shape[0]
    return pl.pallas_call(
        tree_kernel,
        out_shape=[
            jax.ShapeDtypeStruct(((taps_count - 1) * nodes, nodes), BF16),
            jax.ShapeDtypeStruct((nodes, nodes), F32),
            jax.ShapeDtypeStruct((nodes, width), F32),
        ],
        in_specs=whole(len(inputs) + 2),
        out_specs=whole(3),
        cost_estimate=cost(4),
        name="tree",
    )(parents, accepted, *inputs)


def mix_kernel(
    seqs,
    width,
    local_heads,
    keep_bcr_ref,
    got_bcr_ref,
    keep_x_ref,
    got_x_ref,
    links_ref,
    ancestry_ref,
    before_ref,
    taps_x_ref,
    taps_b_ref,
    taps_c_ref,
    bias_ref,
    rate_ref,
    skip_ref,
    state_ref,
    out_ref,
    scale_ref,
    post_x_ref,
    post_b_ref,
    post_c_ref,
):
    nodes, inner = keep_x_ref.shape
    group_cols = taps_b_ref.shape[1]
    head_dim = inner // local_heads
    state_dim = state_ref.shape[3]
    groups = local_heads // HPG
    group_width = HPG * head_dim
    rate_start = 2 * group_cols
    extra = keep_bcr_ref[:, rate_start:].astype(F32) + got_bcr_ref[:, rate_start:].astype(F32)
    scale = lax.rsqrt(extra[:, local_heads : local_heads + 1] / width + EPS)
    scale_ref[...] = jnp.broadcast_to(scale, scale_ref.shape)

    ancestry = ancestry_ref[...]
    step = softplus((extra * scale).astype(BF16).astype(F32) + bias_ref[...])
    decayed = step * rate_ref[...]
    high, rest = split(decayed)
    middle, low = split(rest)
    parts = jnp.concatenate([high, middle, low], axis=1).astype(BF16)
    parts = dot(ancestry.astype(BF16), parts)
    decay = parts[:, :LANES] + parts[:, LANES : 2 * LANES] + parts[:, 2 * LANES :]
    grow = jnp.exp(decay)
    decay_t = decay.T
    step_t = step.T
    is_live = ancestry > 0.5

    def convolve(keep_ref, got_ref, taps_ref, source, start, target_ref):
        last = taps_ref.shape[0] - 1
        for lower in range(0, taps_ref.shape[1], CHUNK):
            span = slice(lower, lower + CHUNK)
            taken = slice(source + lower, source + lower + CHUNK)
            rows = keep_ref[:, taken].astype(F32) + got_ref[:, taken].astype(F32)
            rows = (rows * scale).astype(BF16)
            taps = taps_ref[:, span].astype(F32)
            found = dot(links_ref[...], rows)
            total = before_ref[:, start + lower : start + lower + CHUNK]
            total = total + taps[last : last + 1] * rows.astype(F32)
            for distance in range(1, last + 1):
                total = total + taps[last - distance : last - distance + 1] * found[
                    (distance - 1) * nodes : distance * nodes
                ]
            target_ref[:, span] = silu(total).astype(target_ref.dtype)

    convolve(keep_bcr_ref, got_bcr_ref, taps_b_ref, 0, inner, post_b_ref)
    convolve(keep_bcr_ref, got_bcr_ref, taps_c_ref, group_cols, inner + group_cols, post_c_ref)
    convolve(keep_x_ref, got_x_ref, taps_x_ref, 0, 0, post_x_ref)

    own = lax.rem(lax.broadcasted_iota(jnp.int32, (nodes, 1), 0), seqs)
    per_lanes = LANES // head_dim
    lane_head = lax.broadcasted_iota(jnp.int32, (nodes, LANES), 1) // head_dim
    for group in range(groups):
        rows_c = post_c_ref[:, group * state_dim : (group + 1) * state_dim]
        rows_b = post_b_ref[:, group * state_dim : (group + 1) * state_dim]
        scores = dot_nt(rows_c, rows_b)
        wide_c = rows_c.astype(F32)
        carried = 0.0
        for sequence in range(0, seqs, 2):
            left = jnp.concatenate(
                [
                    jnp.where(own == sequence + place, wide_c, 0.0).astype(BF16)
                    for place in range(2)
                ],
                axis=1,
            )
            right = jnp.concatenate(
                [
                    state_ref[sequence + place, group * HPG : (group + 1) * HPG].reshape(
                        group_width, state_dim
                    )
                    for place in range(2)
                ],
                axis=1,
            )
            carried = carried + dot_nt(left, right)
        for part in range(group_width // LANES):
            start = group * group_width + part * LANES
            rows_x = post_x_ref[:, start : start + LANES]
            half_x = rows_x.astype(BF16)
            within = 0.0
            growth = 0.0
            skip = 0.0
            for place in range(per_lanes):
                head = group * HPG + part * per_lanes + place
                gap = decay[:, head : head + 1] - decay_t[head : head + 1, :nodes]
                mixing = jnp.where(is_live, jnp.exp(jnp.where(is_live, gap, 0.0)), 0.0)
                mixing = (scores * mixing * step_t[head : head + 1, :nodes]).astype(BF16)
                within = jnp.where(lane_head == place, dot(mixing, half_x), within)
                growth = jnp.where(lane_head == place, grow[:, head : head + 1], growth)
                skip = jnp.where(lane_head == place, skip_ref[:, head : head + 1], skip)
            out_ref[:, start : start + LANES] = (
                carried[:, part * LANES : (part + 1) * LANES] * growth
                + within
                + skip * rows_x
            )


def mix(
    seqs,
    width,
    local_heads,
    keep_bcr,
    got_bcr,
    keep_x,
    got_x,
    links,
    ancestry,
    before,
    taps_x,
    taps_b,
    taps_c,
    bias,
    rate,
    skip,
    state,
):
    nodes, inner = keep_x.shape
    operands = [
        keep_bcr,
        got_bcr,
        keep_x,
        got_x,
        links,
        ancestry,
        before,
        taps_x,
        taps_b,
        taps_c,
        bias,
        rate,
        skip,
        state,
    ]
    return pl.pallas_call(
        functools.partial(mix_kernel, seqs, width, local_heads),
        out_shape=[
            jax.ShapeDtypeStruct((nodes, inner), F32),
            jax.ShapeDtypeStruct((nodes, LANES), F32),
        ],
        in_specs=whole(len(operands)),
        out_specs=whole(2),
        scratch_shapes=[
            pltpu.VMEM((nodes, inner), F32),
            pltpu.VMEM((nodes, taps_b.shape[1]), BF16),
            pltpu.VMEM((nodes, taps_c.shape[1]), BF16),
        ],
        cost_estimate=cost(8),
        name="mix",
    )(*operands)


def gate_kernel(group_width, keep_ref, got_ref, scale_ref, heads_ref, gain_ref, out_ref):
    scale = scale_ref[:, :1]
    for lower in range(0, out_ref.shape[1], group_width):
        span = slice(lower, lower + group_width)
        rows = keep_ref[:, span].astype(F32) + got_ref[:, span].astype(F32)
        rows = (rows * scale).astype(BF16).astype(F32)
        gated = heads_ref[:, span] * silu(rows)
        mean = jnp.sum(gated * gated, axis=1, keepdims=True) / group_width
        out_ref[:, span] = (gated * lax.rsqrt(mean + EPS) * gain_ref[:, span]).astype(BF16)


def gate(group_width, keep, got, scale, heads_out, gain):
    return pl.pallas_call(
        functools.partial(gate_kernel, group_width),
        out_shape=jax.ShapeDtypeStruct(heads_out.shape, BF16),
        in_specs=whole(5),
        out_specs=pl.BlockSpec(memory_space=VMEM),
        cost_estimate=cost(1),
        name="gate",
    )(keep, got, scale, heads_out, gain)


def swap_bit(array, bit, blocks):
    return lax.ppermute(array, "kv", [(i, i ^ (1 << bit)) for i in range(blocks)])


def after(value, *others):
    return lax.optimization_barrier((value, *others))[0]


def halving(keep, received, bit, blocks):
    half = keep.shape[0] // 2
    send = (keep[half:].astype(F32) + received[half:].astype(F32)).astype(BF16)

    def stay(*others):
        kept = after(keep, received, send, *others)
        got = after(received, keep, send, *others)
        return kept[:half].astype(F32) + got[:half].astype(F32)

    return send, swap_bit(send, bit, blocks), stay


def mixer(
    kv_count,
    tp_count,
    tokens,
    parents,
    accepted,
    state,
    conv_x,
    conv_b,
    conv_c,
    path_x,
    path_b,
    path_c,
    path_dt,
    gain_in,
    w_x,
    w_z,
    w_b,
    w_c,
    w_dt,
    dt_bias,
    a_log,
    d_skip,
    conv_wx,
    conv_wb,
    conv_wc,
    gain_out,
    w_out,
):
    seq_local = state.shape[0]
    proposals = parents.shape[1]
    heads_local = dt_bias.shape[0]
    head_dim = state.shape[2]
    width = gain_in.shape[0]
    tp_index = lax.axis_index("tp")
    kv_index = lax.axis_index("kv")
    slab_width = tokens.shape[2]
    rows_local = seq_local * proposals
    z_count = tp_count
    x_count = kv_count // z_count
    x_bits = list(range(log2(x_count)))
    z_bits = list(range(log2(x_count), log2(kv_count)))
    x_first = x_bits + z_bits
    z_first = z_bits + x_bits
    z_place = kv_index // x_count

    def by_position(array):
        return array.transpose(1, 0, 2).reshape(-1, array.shape[2])

    tokens_q = tokens.transpose(1, 0, 2).reshape(proposals, kv_count, seq_local, slab_width)
    gains = gain_in[None, :]
    half = kv_count // 2
    of_x = [flipped_bits(position, x_first) for position in range(kv_count)]
    of_z = [flipped_bits(position, z_first) for position in range(kv_count)]
    w_dt_t = w_dt.T
    bcr_args = (tp_count, gains, [w_b, w_c], w_dt_t)
    x_args = (tp_count, gains, [w_x])
    z_args = (tp_count, gains, [w_z])
    send_bcr = project(of_z[half:], tokens_q, *bcr_args)
    got_bcr = swap_bit(send_bcr, z_first[0], kv_count)
    send_x = project(of_x[half:], after(tokens_q, send_bcr), *x_args)
    got_x = swap_bit(send_x, x_first[0], kv_count)
    send_z = project(of_x[half:], after(tokens_q, send_x), *z_args)
    got_z = swap_bit(send_z, x_first[0], kv_count)
    keep_bcr = project(of_z[:half], after(tokens_q, send_z), *bcr_args)
    keep_x = project(of_x[:half], after(tokens_q, keep_bcr), *x_args)

    accepted = accepted[:, None]
    conv_x, conv_b, conv_c = by_position(conv_x), by_position(conv_b), by_position(conv_c)
    path_x, path_b, path_c = by_position(path_x), by_position(path_b), by_position(path_c)
    links, ancestry, before = tree(
        parents,
        after(accepted, keep_x),
        [(conv_x, path_x, conv_wx), (conv_b, path_b, conv_wb), (conv_c, path_c, conv_wc)],
    )
    sent_bcr, got_bcr, stay_bcr = halving(
        keep_bcr, after(got_bcr, links), z_first[1], kv_count
    )
    sent_x, got_x, stay_x = halving(keep_x, after(got_x, sent_bcr), x_first[1], kv_count)
    keep_z = project(of_x[:half], after(tokens_q, sent_x), *z_args)
    a_rate = -jnp.exp(a_log)
    new_state, half_state = replay_state(
        after(accepted, keep_z),
        by_position(path_dt),
        dt_bias[None, :],
        a_log[None, :],
        conv_x,
        path_x,
        conv_wx,
        conv_b,
        path_b,
        conv_wb,
        state,
    )
    keep_bcr = stay_bcr(keep_z)
    keep_x = stay_x(keep_z)
    sent_z, got_z, stay_z = halving(
        keep_z, after(got_z, half_state, keep_bcr, keep_x), x_first[1], kv_count
    )
    for place in range(2, len(x_first)):
        sent_x, got_x, stay_x = halving(
            keep_x, after(got_x, sent_z), x_first[place], kv_count
        )
        sent_bcr, got_bcr, stay_bcr = halving(
            keep_bcr, after(got_bcr, sent_x), z_first[place], kv_count
        )
        keep_x = stay_x(sent_bcr)
        keep_bcr = stay_bcr(sent_bcr)
        keep_z = stay_z(sent_bcr)
        sent_z, got_z, stay_z = halving(
            keep_z, after(got_z, keep_x, keep_bcr), x_first[place], kv_count
        )
    got_x = after(got_x, sent_z)
    got_bcr = after(got_bcr, sent_z)
    keep_z = stay_z(sent_z)

    def padded(values):
        return jnp.pad(values, (0, LANES - heads_local))[None, :]

    heads_out, row_scale = mix(
        seq_local,
        width,
        heads_local,
        keep_bcr,
        got_bcr,
        keep_x,
        got_x,
        links,
        ancestry,
        before,
        conv_wx,
        conv_wb,
        conv_wc,
        padded(dt_bias),
        padded(a_rate),
        d_skip[None, :],
        half_state,
    )
    gated = gate(HPG * head_dim, keep_z, got_z, row_scale, heads_out, gain_out[None, :])

    w_out = after(w_out, sent_bcr, sent_x)
    w_pieces = [w_out]
    for bit in x_bits:
        w_pieces = w_pieces + [swap_bit(piece, bit, kv_count) for piece in w_pieces]
    w_pieces = [after(piece, gated) for piece in w_pieces]
    for bit in x_bits:
        flip = ((kv_index >> bit) & 1) == 1
        w_pieces = [
            jnp.where(flip, w_pieces[place ^ (1 << bit)], w_pieces[place])
            for place in range(x_count)
        ]
    w_block = jnp.concatenate(w_pieces, axis=1)

    pieces = {0: gated}
    for bit in z_bits[::-1]:
        for place in list(pieces):
            pieces[place | (1 << (bit - len(x_bits)))] = swap_bit(pieces[place], bit, kv_count)
    terms = [dot(pieces[place], w_block).astype(BF16) for place in range(z_count)]
    core_flip = ((tp_index ^ z_place) & 1) == 1
    sent = []
    kept = []
    for place in range(0, z_count, 2):
        sent.append(jnp.where(core_flip, terms[place], terms[place + 1]))
        kept.append(jnp.where(core_flip, terms[place + 1], terms[place]))
    swapped = lax.ppermute(
        jnp.concatenate(sent, axis=0), "tp", [(i, i ^ 1) for i in range(tp_count)]
    )
    half = z_count // 2
    paired = (jnp.concatenate(kept, axis=0).astype(F32) + swapped.astype(F32)).astype(
        BF16
    ).reshape(half, rows_local, -1)
    total = 0.0
    for shift in range(half):
        block = (tp_index >> 1) ^ (z_place >> 1) ^ shift
        route = []
        for z in range(z_count):
            for x in range(x_count):
                for t in range(tp_count):
                    z_to = (((t >> 1) ^ shift) << 1) | (t & 1)
                    route.append(
                        ((z * x_count + x) * tp_count + t, (z_to * x_count + x) * tp_count + z)
                    )
        piece = lax.dynamic_index_in_dim(paired, block, 0, keepdims=False)
        total = total + lax.ppermute(piece, ("kv", "tp"), route).astype(F32)
    mixed = total.astype(BF16).reshape(proposals, seq_local, -1).transpose(1, 0, 2)
    return (mixed, new_state)


def solution(mesh):
    return jax.shard_map(
        functools.partial(mixer, mesh.shape["kv"], mesh.shape["tp"]),
        mesh=mesh,
        in_specs=(
            P(None, None, "kv"),
            P("kv", None),
            P("kv"),
            P("kv", "tp", None, None),
            P("kv", None, "tp"),
            P("kv", None, "tp"),
            P("kv", None, "tp"),
            P("kv", None, "tp"),
            P("kv", None, "tp"),
            P("kv", None, "tp"),
            P("kv", None, "tp"),
            P(),
            P("kv", "tp"),
            P("kv", "tp"),
            P("kv", "tp"),
            P("kv", "tp"),
            P(),
            P("tp"),
            P("tp"),
            P("tp"),
            P(None, "tp"),
            P(None, "tp"),
            P(None, "tp"),
            P("tp"),
            P("tp", "kv"),
        ),
        out_specs=(P("kv", None, "tp"), P("kv", "tp", None, None)),
        check_vma=False,
    )
```

```python
import functools

import jax
import jax.numpy as jnp
from jax import lax
from jax.experimental import pallas as pl
from jax.experimental.pallas import tpu as pltpu
from jax.sharding import PartitionSpec as P


HPG = 4
EPS = 1e-06
LANES = 128
CHUNK = 256
VMEM = pltpu.VMEM
F32 = jnp.float32
BF16 = jnp.bfloat16
NT = (((1,), (1,)), ((), ()))


def log2(count):
    return count.bit_length() - 1


def flipped_bits(position, order):
    value = 0
    for place, bit in enumerate(order):
        value |= ((position >> (len(order) - 1 - place)) & 1) << bit
    return value


def whole(count):
    return [pl.BlockSpec(memory_space=VMEM) for _ in range(count)]


def cost(microseconds):
    return pl.CostEstimate(
        flops=int(microseconds * 4e6), bytes_accessed=1024, transcendentals=0
    )


def dot(left, right):
    return jnp.dot(left, right, preferred_element_type=F32)


def dot_nt(left, right):
    return lax.dot_general(left, right, NT, preferred_element_type=F32)


def silu(values):
    return values / (1.0 + jnp.exp(-values))


def softplus(values):
    return jnp.maximum(values, 0.0) + jnp.log1p(jnp.exp(-jnp.abs(values)))


def project_kernel(differences, with_rate, tp_count, tokens_ref, gain_ref, *refs):
    props, _, seqs, width = tokens_ref.shape
    me = lax.axis_index("kv")
    rows_local = props * seqs
    if with_rate:
        w_dt_ref, *w_refs, out_ref, scaled_ref, squares_ref = refs
    else:
        *w_refs, out_ref, scaled_ref = refs
    slab_start = pl.multiple_of(me * width, LANES)
    gain = gain_ref[:, pl.ds(slab_start, width)]
    for position, difference in enumerate(differences):
        rows = tokens_ref[:, me ^ difference].astype(F32).reshape(rows_local, width)
        span = slice(position * rows_local, (position + 1) * rows_local)
        scaled_ref[span] = (rows * gain).astype(BF16)
        if with_rate:
            squares_ref[span] = jnp.sum(rows * rows, axis=1, keepdims=True)
    start = 0
    for w_ref in w_refs:
        for lower in range(0, w_ref.shape[1], CHUNK):
            upper = min(lower + CHUNK, w_ref.shape[1])
            out_ref[:, start + lower : start + upper] = dot(
                scaled_ref[...], w_ref[:, lower:upper]
            ).astype(BF16)
        start += w_ref.shape[1]
    if with_rate:
        heads = w_dt_ref.shape[0]
        local = heads // tp_count
        first = lax.axis_index("tp") * local
        row = lax.broadcasted_iota(jnp.int32, (LANES, heads), 0)
        column = lax.broadcasted_iota(jnp.int32, (LANES, heads), 1)
        pick = jnp.where((row < local) & (column == row + first), 1.0, 0.0).astype(BF16)
        slab = w_dt_ref[:, pl.ds(slab_start, width)]
        w_rate = dot(pick, slab).astype(BF16)
        lane = lax.broadcasted_iota(jnp.int32, (1, LANES), 1)
        rate = dot_nt(scaled_ref[...], w_rate)
        out_ref[:, start : start + LANES] = jnp.where(
            lane == local, squares_ref[...], rate
        ).astype(BF16)


def project(differences, tokens, tp_count, gain, weights, w_dt=None):
    props, _, seqs, width = tokens.shape
    rows = len(differences) * props * seqs
    columns = sum(weight.shape[1] for weight in weights)
    scratch = [pltpu.VMEM((rows, width), BF16)]
    operands = [tokens, gain]
    if w_dt is not None:
        columns += LANES
        scratch.append(pltpu.VMEM((rows, 1), F32))
        operands.append(w_dt)
    operands += list(weights)
    return pl.pallas_call(
        functools.partial(project_kernel, tuple(differences), w_dt is not None, tp_count),
        out_shape=jax.ShapeDtypeStruct((rows, columns), BF16),
        in_specs=whole(len(operands)),
        out_specs=pl.BlockSpec(memory_space=VMEM),
        scratch_shapes=scratch,
        cost_estimate=cost(2),
    )(*operands)


def window(conv_ref, path_ref, taps_ref, seqs):
    history = jnp.concatenate([conv_ref[...].astype(F32), path_ref[...].astype(F32)], axis=0)
    count = path_ref.shape[0]
    taps = taps_ref[...].astype(F32)
    total = taps[0:1] * history[0:count]
    for distance in range(1, taps.shape[0]):
        total = total + taps[distance : distance + 1] * history[
            distance * seqs : distance * seqs + count
        ]
    return silu(total)


def as_column(row):
    count = row.shape[1]
    place = lax.broadcasted_iota(jnp.int32, (count, count), 0)
    other = lax.broadcasted_iota(jnp.int32, (count, count), 1)
    return jnp.sum(jnp.where(place == other, row, 0), axis=1, keepdims=True)


def split(values):
    high = values.astype(BF16).astype(F32)
    return high, values - high


def state_kernel(
    accepted_ref,
    path_dt_ref,
    bias_ref,
    a_log_ref,
    conv_x_ref,
    path_x_ref,
    taps_x_ref,
    conv_b_ref,
    path_b_ref,
    taps_b_ref,
    state_ref,
    out_ref,
    half_ref,
    left_ref,
    right_ref,
    decay_ref,
):
    _, heads, head_dim, state_dim = state_ref.shape
    seqs = accepted_ref.shape[1]
    sequence = pl.program_id(0)
    count = path_x_ref.shape[0]
    group_width = HPG * head_dim

    @pl.when(sequence == 0)
    def _():
        lane = lax.broadcasted_iota(jnp.int32, (heads, heads * head_dim), 1)
        row = lax.broadcasted_iota(jnp.int32, (heads, heads * head_dim), 0)
        spread = jnp.where(lane // head_dim == row, 1.0, 0.0).astype(BF16)
        accepted = as_column(accepted_ref[...])
        a_rate = -jnp.exp(a_log_ref[...])
        steps = softplus(path_dt_ref[...].astype(F32) + bias_ref[...])
        weights = []
        overall = jnp.zeros((seqs, heads), F32)
        for position in range(count // seqs - 1, -1, -1):
            step = steps[position * seqs : (position + 1) * seqs]
            live = jnp.where(position < accepted, 1.0, 0.0)
            weights.append(live * jnp.exp(overall) * step)
            overall = overall + step * a_rate * live
        decay_ref[...] = jnp.exp(overall)
        high, low = split(jnp.concatenate(weights[::-1], axis=0))
        weights = dot(high.astype(BF16), spread) + dot(low.astype(BF16), spread)
        grown = weights * window(conv_x_ref, path_x_ref, taps_x_ref, seqs)
        empty = jnp.zeros((LANES - 2 * count, grown.shape[1]), F32)
        turned = jnp.concatenate([grown, grown, empty], axis=0).T
        high, low = split(turned)
        left_ref[:, :LANES] = high.astype(BF16)
        left_ref[:, LANES:] = low.astype(BF16)
        rows_b = window(conv_b_ref, path_b_ref, taps_b_ref, seqs)
        high, low = split(rows_b)
        right_ref[...] = jnp.zeros_like(right_ref)
        right_ref[0:count] = high
        right_ref[count : 2 * count] = low
        right_ref[LANES : LANES + count] = high

    row = lax.broadcasted_iota(jnp.int32, (2 * LANES, 1), 0)
    mine = jnp.where(lax.rem(row, seqs) == sequence, 1.0, 0.0)
    right = (right_ref[...] * mine).astype(BF16)
    decay = decay_ref[pl.ds(sequence, 1), :]
    for group in range(heads // HPG):
        grown = dot(
            left_ref[group * group_width : (group + 1) * group_width],
            right[:, group * state_dim : (group + 1) * state_dim],
        )
        for head in range(HPG):
            index = group * HPG + head
            value = decay[:, index : index + 1] * state_ref[0, index] + grown[
                head * head_dim : (head + 1) * head_dim
            ]
            out_ref[0, index] = value
            half_ref[0, index] = value.astype(BF16)


def replay_state(accepted, path_dt, bias, a_log, conv_x, path_x, taps_x, conv_b, path_b, taps_b, state):
    seqs, heads, head_dim, state_dim = state.shape
    block = pl.BlockSpec((1, heads, head_dim, state_dim), lambda s: (s, 0, 0, 0))

    def full(array):
        return pl.BlockSpec(array.shape, lambda s: (0,) * array.ndim)

    small = [accepted, path_dt, bias, a_log, conv_x, path_x, taps_x, conv_b, path_b, taps_b]
    return pl.pallas_call(
        state_kernel,
        grid=(seqs,),
        out_shape=[
            jax.ShapeDtypeStruct(state.shape, F32),
            jax.ShapeDtypeStruct(state.shape, BF16),
        ],
        in_specs=[full(a) for a in small] + [block],
        out_specs=[block, block],
        scratch_shapes=[
            pltpu.VMEM((heads * head_dim, 2 * LANES), BF16),
            pltpu.VMEM((2 * LANES, path_b.shape[1]), F32),
            pltpu.VMEM((seqs, heads), F32),
        ],
        cost_estimate=cost(8),
        name="replay_state",
    )(*small, state)


def tree_kernel(parents_ref, accepted_ref, *refs):
    *inputs, links_ref, ancestry_ref, before_ref = refs
    seqs, props = parents_ref.shape
    nodes = seqs * props
    parents = parents_ref[...]
    parent = jnp.concatenate([parents[:, place : place + 1] for place in range(props)], axis=0)
    accepted = jnp.concatenate([as_column(accepted_ref[...])] * props, axis=0)
    row = lax.broadcasted_iota(jnp.int32, (nodes, nodes), 0)
    column = lax.broadcasted_iota(jnp.int32, (nodes, nodes), 1)
    own = lax.rem(lax.broadcasted_iota(jnp.int32, (nodes, 1), 0), seqs)
    target = jnp.where(parent >= 0, parent * seqs + own, -1)
    link = jnp.where(column == target, 1.0, 0.0)
    ancestry = link + jnp.where(row == column, 1.0, 0.0)
    link = link.astype(BF16)
    reach = link
    taps_count = inputs[2].shape[0]
    for distance in range(1, taps_count):
        links_ref[(distance - 1) * nodes : distance * nodes] = reach
        reach = dot(reach, link).astype(BF16)
    for _ in range(props.bit_length()):
        half = ancestry.astype(BF16)
        ancestry = jnp.minimum(dot(half, half), 1.0)
    ancestry_ref[...] = ancestry
    depth = jnp.sum(ancestry, axis=1, keepdims=True).astype(jnp.int32) - 1
    last = taps_count - 1

    def chosen(first, rows, distance):
        lane = lax.broadcasted_iota(jnp.int32, (nodes, rows), 1)
        wanted = accepted + last - distance + depth
        hit = (lane // seqs + first == wanted) & (lax.rem(lane, seqs) == own)
        return jnp.where(hit & (depth < distance), 1.0, 0.0).astype(BF16)

    conv_rows = inputs[0].shape[0]
    path_rows = inputs[1].shape[0]
    picks = [
        (chosen(0, conv_rows, d), chosen(conv_rows // seqs, path_rows, d))
        for d in range(1, taps_count)
    ]
    start = 0
    for which in range(0, len(inputs), 3):
        conv_ref, path_ref, taps_ref = inputs[which : which + 3]
        taps = taps_ref[...].astype(F32)
        total = 0.0
        for distance in range(1, taps_count):
            early, late = picks[distance - 1]
            found = dot(early, conv_ref[...]) + dot(late, path_ref[...])
            total = total + taps[last - distance : last - distance + 1] * found
        before_ref[:, start : start + conv_ref.shape[1]] = total
        start += conv_ref.shape[1]


def tree(parents, accepted, streams):
    nodes = parents.shape[0] * parents.shape[1]
    inputs = [array for stream in streams for array in stream]
    width = sum(stream[0].shape[1] for stream in streams)
    taps_count = streams[0][2].shape[0]
    return pl.pallas_call(
        tree_kernel,
        out_shape=[
            jax.ShapeDtypeStruct(((taps_count - 1) * nodes, nodes), BF16),
            jax.ShapeDtypeStruct((nodes, nodes), F32),
            jax.ShapeDtypeStruct((nodes, width), F32),
        ],
        in_specs=whole(len(inputs) + 2),
        out_specs=whole(3),
        cost_estimate=cost(4),
        name="tree",
    )(parents, accepted, *inputs)


def added(refs, span):
    return sum(ref[:, span].astype(F32) for ref in refs)


def mix_kernel(
    seqs,
    width,
    local_heads,
    addends,
    *refs,
):
    bcr_refs = refs[:addends]
    x_refs = refs[addends : 2 * addends]
    (
        links_ref,
        ancestry_ref,
        before_ref,
        taps_x_ref,
        taps_b_ref,
        taps_c_ref,
        bias_ref,
        a_log_ref,
        skip_ref,
        state_ref,
        out_ref,
        scale_ref,
        post_x_ref,
        post_b_ref,
        post_c_ref,
    ) = refs[2 * addends :]
    nodes, inner = x_refs[0].shape
    group_cols = taps_b_ref.shape[1]
    head_dim = inner // local_heads
    state_dim = state_ref.shape[3]
    groups = local_heads // HPG
    group_width = HPG * head_dim
    rate_start = 2 * group_cols
    extra = added(bcr_refs, slice(rate_start, rate_start + LANES))
    empty = jnp.zeros((1, LANES - local_heads), F32)
    bias = jnp.concatenate([bias_ref[...], empty], axis=1)
    a_rate = jnp.concatenate([-jnp.exp(a_log_ref[...]), empty], axis=1)
    scale = lax.rsqrt(extra[:, local_heads : local_heads + 1] / width + EPS)
    scale_ref[...] = jnp.broadcast_to(scale, scale_ref.shape)

    ancestry = ancestry_ref[...]
    step = softplus((extra * scale).astype(BF16).astype(F32) + bias)
    decayed = step * a_rate
    high, rest = split(decayed)
    middle, low = split(rest)
    parts = jnp.concatenate([high, middle, low], axis=1).astype(BF16)
    parts = dot(ancestry.astype(BF16), parts)
    decay = parts[:, :LANES] + parts[:, LANES : 2 * LANES] + parts[:, 2 * LANES :]
    grow = jnp.exp(decay)
    decay_t = decay.T
    step_t = step.T
    is_live = ancestry > 0.5

    def convolve(row_refs, taps_ref, source, start, target_ref):
        last = taps_ref.shape[0] - 1
        for lower in range(0, taps_ref.shape[1], CHUNK):
            span = slice(lower, lower + CHUNK)
            rows = added(row_refs, slice(source + lower, source + lower + CHUNK))
            rows = (rows * scale).astype(BF16)
            taps = taps_ref[:, span].astype(F32)
            found = dot(links_ref[...], rows)
            total = before_ref[:, start + lower : start + lower + CHUNK]
            total = total + taps[last : last + 1] * rows.astype(F32)
            for distance in range(1, last + 1):
                total = total + taps[last - distance : last - distance + 1] * found[
                    (distance - 1) * nodes : distance * nodes
                ]
            target_ref[:, span] = silu(total).astype(target_ref.dtype)

    convolve(bcr_refs, taps_b_ref, 0, inner, post_b_ref)
    convolve(bcr_refs, taps_c_ref, group_cols, inner + group_cols, post_c_ref)
    convolve(x_refs, taps_x_ref, 0, 0, post_x_ref)

    own = lax.rem(lax.broadcasted_iota(jnp.int32, (nodes, 1), 0), seqs)
    per_lanes = LANES // head_dim
    lane_head = lax.broadcasted_iota(jnp.int32, (nodes, LANES), 1) // head_dim
    for group in range(groups):
        rows_c = post_c_ref[:, group * state_dim : (group + 1) * state_dim]
        rows_b = post_b_ref[:, group * state_dim : (group + 1) * state_dim]
        scores = dot_nt(rows_c, rows_b)
        wide_c = rows_c.astype(F32)
        carried = 0.0
        for sequence in range(0, seqs, 2):
            left = jnp.concatenate(
                [
                    jnp.where(own == sequence + place, wide_c, 0.0).astype(BF16)
                    for place in range(2)
                ],
                axis=1,
            )
            right = jnp.concatenate(
                [
                    state_ref[sequence + place, group * HPG : (group + 1) * HPG].reshape(
                        group_width, state_dim
                    )
                    for place in range(2)
                ],
                axis=1,
            )
            carried = carried + dot_nt(left, right)
        for part in range(group_width // LANES):
            start = group * group_width + part * LANES
            rows_x = post_x_ref[:, start : start + LANES]
            half_x = rows_x.astype(BF16)
            within = 0.0
            growth = 0.0
            skip = 0.0
            for place in range(per_lanes):
                head = group * HPG + part * per_lanes + place
                gap = decay[:, head : head + 1] - decay_t[head : head + 1, :nodes]
                mixing = jnp.where(is_live, jnp.exp(jnp.where(is_live, gap, 0.0)), 0.0)
                mixing = (scores * mixing * step_t[head : head + 1, :nodes]).astype(BF16)
                within = jnp.where(lane_head == place, dot(mixing, half_x), within)
                growth = jnp.where(lane_head == place, grow[:, head : head + 1], growth)
                skip = jnp.where(lane_head == place, skip_ref[:, head : head + 1], skip)
            out_ref[:, start : start + LANES] = (
                carried[:, part * LANES : (part + 1) * LANES] * growth
                + within
                + skip * rows_x
            )


def first_rows(arrays, nodes):
    return [pl.BlockSpec((nodes, array.shape[1]), lambda i: (0, 0)) for array in arrays]


def full_blocks(arrays):
    return [
        pl.BlockSpec(array.shape, functools.partial(lambda rank, i: (0,) * rank, array.ndim))
        for array in arrays
    ]


def mix(seqs, width, local_heads, bcr, x, others):
    nodes, inner = x[-1].shape
    group_cols = others[4].shape[1]
    outs = [
        jax.ShapeDtypeStruct((nodes, inner), F32),
        jax.ShapeDtypeStruct((nodes, LANES), F32),
    ]
    return pl.pallas_call(
        functools.partial(mix_kernel, seqs, width, local_heads, len(x)),
        grid=(1,),
        out_shape=outs,
        in_specs=first_rows(bcr + x, nodes) + full_blocks(others),
        out_specs=full_blocks(outs),
        scratch_shapes=[
            pltpu.VMEM((nodes, inner), F32),
            pltpu.VMEM((nodes, group_cols), BF16),
            pltpu.VMEM((nodes, group_cols), BF16),
        ],
        cost_estimate=cost(8),
        name="mix",
    )(*bcr, *x, *others)


def gate_kernel(group_width, *refs):
    *row_refs, scale_ref, heads_ref, gain_ref, out_ref = refs
    scale = scale_ref[:, :1]
    for lower in range(0, out_ref.shape[1], group_width):
        span = slice(lower, lower + group_width)
        rows = (added(row_refs, span) * scale).astype(BF16).astype(F32)
        gated = heads_ref[:, span] * silu(rows)
        mean = jnp.sum(gated * gated, axis=1, keepdims=True) / group_width
        out_ref[:, span] = (gated * lax.rsqrt(mean + EPS) * gain_ref[:, span]).astype(BF16)


def gate(group_width, rows, scale, heads_out, gain):
    out = jax.ShapeDtypeStruct(heads_out.shape, BF16)
    return pl.pallas_call(
        functools.partial(gate_kernel, group_width),
        grid=(1,),
        out_shape=out,
        in_specs=first_rows(rows, heads_out.shape[0]) + full_blocks([scale, heads_out, gain]),
        out_specs=full_blocks([out])[0],
        cost_estimate=cost(1),
        name="gate",
    )(*rows, scale, heads_out, gain)


def swap_bit(array, bit, blocks):
    return lax.ppermute(array, "kv", [(i, i ^ (1 << bit)) for i in range(blocks)])


def after(value, *others):
    return lax.optimization_barrier((value, *others))[0]


def halving(addends, bit, blocks, *others):
    half = addends[-1].shape[0] // 2
    addends = [*addends[:-1], after(addends[-1], *others)]
    send = sum(addend[half : 2 * half].astype(F32) for addend in addends).astype(BF16)
    return send, [*addends, swap_bit(send, bit, blocks)]


def mixer(
    kv_count,
    tp_count,
    tokens,
    parents,
    accepted,
    state,
    conv_x,
    conv_b,
    conv_c,
    path_x,
    path_b,
    path_c,
    path_dt,
    gain_in,
    w_x,
    w_z,
    w_b,
    w_c,
    w_dt,
    dt_bias,
    a_log,
    d_skip,
    conv_wx,
    conv_wb,
    conv_wc,
    gain_out,
    w_out,
):
    seq_local = state.shape[0]
    proposals = parents.shape[1]
    heads_local = dt_bias.shape[0]
    head_dim = state.shape[2]
    width = gain_in.shape[0]
    tp_index = lax.axis_index("tp")
    kv_index = lax.axis_index("kv")
    slab_width = tokens.shape[2]
    rows_local = seq_local * proposals
    z_count = tp_count
    x_count = kv_count // z_count
    x_bits = list(range(log2(x_count)))
    z_bits = list(range(log2(x_count), log2(kv_count)))
    x_first = x_bits + z_bits
    z_first = z_bits + x_bits
    z_place = kv_index // x_count

    def by_position(array):
        return array.transpose(1, 0, 2).reshape(-1, array.shape[2])

    tokens_q = tokens.transpose(1, 0, 2).reshape(proposals, kv_count, seq_local, slab_width)
    gains = gain_in[None, :]
    half = kv_count // 2
    of_x = [flipped_bits(position, x_first) for position in range(kv_count)]
    of_z = [flipped_bits(position, z_first) for position in range(kv_count)]
    w_dt_t = w_dt.T
    bcr_args = (tp_count, gains, [w_b, w_c], w_dt_t)
    x_args = (tp_count, gains, [w_x])
    z_args = (tp_count, gains, [w_z])
    send_bcr = project(of_z[half:], tokens_q, *bcr_args)
    got_bcr = swap_bit(send_bcr, z_first[0], kv_count)
    send_x = project(of_x[half:], after(tokens_q, send_bcr), *x_args)
    got_x = swap_bit(send_x, x_first[0], kv_count)
    send_z = project(of_x[half:], after(tokens_q, send_x), *z_args)
    got_z = swap_bit(send_z, x_first[0], kv_count)
    keep_bcr = project(of_z[:half], after(tokens_q, send_z), *bcr_args)
    keep_x = project(of_x[:half], after(tokens_q, keep_bcr), *x_args)

    accepted = accepted[None, :]
    conv_x, conv_b, conv_c = by_position(conv_x), by_position(conv_b), by_position(conv_c)
    path_x, path_b, path_c = by_position(path_x), by_position(path_b), by_position(path_c)
    links, ancestry, before = tree(
        parents,
        after(accepted, keep_x),
        [(conv_x, path_x, conv_wx), (conv_b, path_b, conv_wb), (conv_c, path_c, conv_wc)],
    )
    sent_bcr, bcr = halving([keep_bcr, got_bcr], z_first[1], kv_count, links)
    sent_x, x = halving([keep_x, got_x], x_first[1], kv_count, sent_bcr)
    keep_z = project(of_x[:half], after(tokens_q, sent_x), *z_args)
    new_state, half_state = replay_state(
        after(accepted, keep_z),
        by_position(path_dt),
        dt_bias[None, :],
        a_log[None, :],
        conv_x,
        path_x,
        conv_wx,
        conv_b,
        path_b,
        conv_wb,
        state,
    )
    sent_z, z = halving([keep_z, got_z], x_first[1], kv_count, half_state)
    for place in range(2, len(x_first)):
        sent_x, x = halving(x, x_first[place], kv_count, sent_z)
        sent_bcr, bcr = halving(bcr, z_first[place], kv_count, sent_x)
        sent_z, z = halving(z, x_first[place], kv_count, sent_bcr)

    heads_out, row_scale = mix(
        seq_local,
        width,
        heads_local,
        [*bcr[:-1], after(bcr[-1], sent_z)],
        [*x[:-1], after(x[-1], sent_z)],
        [
            links,
            ancestry,
            before,
            conv_wx,
            conv_wb,
            conv_wc,
            dt_bias[None, :],
            a_log[None, :],
            d_skip[None, :],
            half_state,
        ],
    )
    gated = gate(HPG * head_dim, z, row_scale, heads_out, gain_out[None, :])

    w_out = after(w_out, sent_bcr, sent_x)
    w_pieces = [w_out]
    for bit in x_bits:
        w_pieces = w_pieces + [swap_bit(piece, bit, kv_count) for piece in w_pieces]
    w_pieces = [after(piece, gated) for piece in w_pieces]
    for bit in x_bits:
        flip = ((kv_index >> bit) & 1) == 1
        w_pieces = [
            jnp.where(flip, w_pieces[place ^ (1 << bit)], w_pieces[place])
            for place in range(x_count)
        ]
    w_block = jnp.concatenate(w_pieces, axis=1)

    pieces = {0: gated}
    for bit in z_bits[::-1]:
        for place in list(pieces):
            pieces[place | (1 << (bit - len(x_bits)))] = swap_bit(pieces[place], bit, kv_count)
    terms = [dot(pieces[place], w_block).astype(BF16) for place in range(z_count)]
    core_flip = ((tp_index ^ z_place) & 1) == 1
    sent = []
    kept = []
    for place in range(0, z_count, 2):
        sent.append(jnp.where(core_flip, terms[place], terms[place + 1]))
        kept.append(jnp.where(core_flip, terms[place + 1], terms[place]))
    swapped = lax.ppermute(
        jnp.concatenate(sent, axis=0), "tp", [(i, i ^ 1) for i in range(tp_count)]
    )
    half = z_count // 2
    paired = (jnp.concatenate(kept, axis=0).astype(F32) + swapped.astype(F32)).astype(
        BF16
    ).reshape(half, rows_local, -1)
    total = 0.0
    for shift in range(half):
        block = (tp_index >> 1) ^ (z_place >> 1) ^ shift
        route = []
        for z in range(z_count):
            for x in range(x_count):
                for t in range(tp_count):
                    z_to = (((t >> 1) ^ shift) << 1) | (t & 1)
                    route.append(
                        ((z * x_count + x) * tp_count + t, (z_to * x_count + x) * tp_count + z)
                    )
        piece = lax.dynamic_index_in_dim(paired, block, 0, keepdims=False)
        total = total + lax.ppermute(piece, ("kv", "tp"), route).astype(F32)
    mixed = total.astype(BF16).reshape(proposals, seq_local, -1).transpose(1, 0, 2)
    return (mixed, new_state)


def solution(mesh):
    return jax.shard_map(
        functools.partial(mixer, mesh.shape["kv"], mesh.shape["tp"]),
        mesh=mesh,
        in_specs=(
            P(None, None, "kv"),
            P("kv", None),
            P("kv"),
            P("kv", "tp", None, None),
            P("kv", None, "tp"),
            P("kv", None, "tp"),
            P("kv", None, "tp"),
            P("kv", None, "tp"),
            P("kv", None, "tp"),
            P("kv", None, "tp"),
            P("kv", None, "tp"),
            P(),
            P("kv", "tp"),
            P("kv", "tp"),
            P("kv", "tp"),
            P("kv", "tp"),
            P(),
            P("tp"),
            P("tp"),
            P("tp"),
            P(None, "tp"),
            P(None, "tp"),
            P(None, "tp"),
            P("tp"),
            P("tp", "kv"),
        ),
        out_specs=(P("kv", None, "tp"), P("kv", "tp", None, None)),
        check_vma=False,
    )
```

```python
import functools

import jax
import jax.numpy as jnp
from jax import lax
from jax.experimental import pallas as pl
from jax.experimental.pallas import tpu as pltpu
from jax.sharding import PartitionSpec as P


HPG = 4
EPS = 1e-06
LANES = 128
CHUNK = 256
RATE_ROWS = 32
VMEM = pltpu.VMEM
F32 = jnp.float32
BF16 = jnp.bfloat16
NT = (((1,), (1,)), ((), ()))


def log2(count):
    return count.bit_length() - 1


def flipped_bits(position, order):
    value = 0
    for place, bit in enumerate(order):
        value |= ((position >> (len(order) - 1 - place)) & 1) << bit
    return value


def whole(count):
    return [pl.BlockSpec(memory_space=VMEM) for _ in range(count)]


def cost(microseconds):
    return pl.CostEstimate(
        flops=int(microseconds * 4e6), bytes_accessed=1024, transcendentals=0
    )


def dot(left, right):
    return jnp.dot(left, right, preferred_element_type=F32)


def dot_nt(left, right):
    return lax.dot_general(left, right, NT, preferred_element_type=F32)


def silu(values):
    return values / (1.0 + jnp.exp(-values))


def softplus(values):
    return jnp.maximum(values, 0.0) + jnp.log1p(jnp.exp(-jnp.abs(values)))


def project_kernel(differences, with_rate, tp_count, tokens_ref, gain_ref, *refs):
    props, _, seqs, width = tokens_ref.shape
    me = lax.axis_index("kv")
    rows_local = props * seqs
    if with_rate:
        w_dt_ref, *w_refs, out_ref, rate_ref, scaled_ref, squares_ref = refs
    else:
        *w_refs, out_ref, scaled_ref = refs
    slab_start = pl.multiple_of(me * width, LANES)
    gain = gain_ref[:, pl.ds(slab_start, width)]
    for position, difference in enumerate(differences):
        rows = tokens_ref[:, me ^ difference].astype(F32).reshape(rows_local, width)
        span = slice(position * rows_local, (position + 1) * rows_local)
        scaled_ref[span] = (rows * gain).astype(BF16)
        if with_rate:
            high, low = split(rows * rows)
            squares_ref[0, span] = high.astype(BF16)
            squares_ref[1, span] = low.astype(BF16)
    start = 0
    for w_ref in w_refs:
        for lower in range(0, w_ref.shape[1], CHUNK):
            upper = min(lower + CHUNK, w_ref.shape[1])
            out_ref[:, start + lower : start + upper] = dot(
                scaled_ref[...], w_ref[:, lower:upper]
            ).astype(BF16)
        start += w_ref.shape[1]
    if with_rate:
        heads = w_dt_ref.shape[0]
        local = heads // tp_count
        first = lax.axis_index("tp") * local
        row = lax.broadcasted_iota(jnp.int32, (RATE_ROWS, heads), 0)
        column = lax.broadcasted_iota(jnp.int32, (RATE_ROWS, heads), 1)
        pick = jnp.where((row < local) & (column == row + first), 1.0, 0.0).astype(BF16)
        slab = w_dt_ref[:, pl.ds(slab_start, width)]
        w_rate = dot(pick, slab).astype(BF16)
        ones = jnp.ones((RATE_ROWS, width), BF16)
        squares = dot_nt(ones, squares_ref[0]) + dot_nt(ones, squares_ref[1])
        out_row = lax.broadcasted_iota(jnp.int32, (RATE_ROWS, 1), 0)
        rate = dot_nt(w_rate, scaled_ref[...])
        rate_ref[...] = jnp.where(out_row == local, squares, rate).astype(BF16)


def project(differences, tokens, tp_count, gain, weights, w_dt=None):
    props, _, seqs, width = tokens.shape
    rows = len(differences) * props * seqs
    columns = sum(weight.shape[1] for weight in weights)
    outs = [jax.ShapeDtypeStruct((rows, columns), BF16)]
    scratch = [pltpu.VMEM((rows, width), BF16)]
    operands = [tokens, gain]
    if w_dt is not None:
        outs.append(jax.ShapeDtypeStruct((RATE_ROWS, rows), BF16))
        scratch.append(pltpu.VMEM((2, rows, width), BF16))
        operands.append(w_dt)
    operands += list(weights)
    return pl.pallas_call(
        functools.partial(project_kernel, tuple(differences), w_dt is not None, tp_count),
        out_shape=outs,
        in_specs=whole(len(operands)),
        out_specs=whole(len(outs)),
        scratch_shapes=scratch,
        cost_estimate=cost(2),
    )(*operands)


def window(conv_ref, path_ref, taps_ref, seqs):
    history = jnp.concatenate([conv_ref[...].astype(F32), path_ref[...].astype(F32)], axis=0)
    count = path_ref.shape[0]
    taps = taps_ref[...].astype(F32)
    total = taps[0:1] * history[0:count]
    for distance in range(1, taps.shape[0]):
        total = total + taps[distance : distance + 1] * history[
            distance * seqs : distance * seqs + count
        ]
    return silu(total)


def as_column(row):
    count = row.shape[1]
    place = lax.broadcasted_iota(jnp.int32, (count, count), 0)
    other = lax.broadcasted_iota(jnp.int32, (count, count), 1)
    return jnp.sum(jnp.where(place == other, row, 0), axis=1, keepdims=True)


def split(values):
    high = values.astype(BF16).astype(F32)
    return high, values - high


def state_kernel(
    accepted_ref,
    path_dt_ref,
    bias_ref,
    a_log_ref,
    conv_x_ref,
    path_x_ref,
    taps_x_ref,
    conv_b_ref,
    path_b_ref,
    taps_b_ref,
    state_ref,
    out_ref,
    half_ref,
    left_ref,
    right_ref,
    decay_ref,
):
    _, heads, head_dim, state_dim = state_ref.shape
    seqs = accepted_ref.shape[1]
    sequence = pl.program_id(0)
    count = path_x_ref.shape[0]
    group_width = HPG * head_dim

    @pl.when(sequence == 0)
    def _():
        lane = lax.broadcasted_iota(jnp.int32, (heads, heads * head_dim), 1)
        row = lax.broadcasted_iota(jnp.int32, (heads, heads * head_dim), 0)
        spread = jnp.where(lane // head_dim == row, 1.0, 0.0).astype(BF16)
        accepted = as_column(accepted_ref[...])
        a_rate = -jnp.exp(a_log_ref[...])
        steps = softplus(path_dt_ref[...].astype(F32) + bias_ref[...])
        weights = []
        overall = jnp.zeros((seqs, heads), F32)
        for position in range(count // seqs - 1, -1, -1):
            step = steps[position * seqs : (position + 1) * seqs]
            live = jnp.where(position < accepted, 1.0, 0.0)
            weights.append(live * jnp.exp(overall) * step)
            overall = overall + step * a_rate * live
        decay_ref[...] = jnp.exp(overall)
        high, low = split(jnp.concatenate(weights[::-1], axis=0))
        weights = dot(high.astype(BF16), spread) + dot(low.astype(BF16), spread)
        grown = weights * window(conv_x_ref, path_x_ref, taps_x_ref, seqs)
        empty = jnp.zeros((LANES - 2 * count, grown.shape[1]), F32)
        turned = jnp.concatenate([grown, grown, empty], axis=0).T
        high, low = split(turned)
        left_ref[:, :LANES] = high.astype(BF16)
        left_ref[:, LANES:] = low.astype(BF16)
        rows_b = window(conv_b_ref, path_b_ref, taps_b_ref, seqs)
        high, low = split(rows_b)
        right_ref[...] = jnp.zeros_like(right_ref)
        right_ref[0:count] = high
        right_ref[count : 2 * count] = low
        right_ref[LANES : LANES + count] = high

    row = lax.broadcasted_iota(jnp.int32, (2 * LANES, 1), 0)
    mine = jnp.where(lax.rem(row, seqs) == sequence, 1.0, 0.0)
    right = (right_ref[...] * mine).astype(BF16)
    decay = decay_ref[pl.ds(sequence, 1), :]
    for group in range(heads // HPG):
        grown = dot(
            left_ref[group * group_width : (group + 1) * group_width],
            right[:, group * state_dim : (group + 1) * state_dim],
        )
        for head in range(HPG):
            index = group * HPG + head
            value = decay[:, index : index + 1] * state_ref[0, index] + grown[
                head * head_dim : (head + 1) * head_dim
            ]
            out_ref[0, index] = value
            half_ref[0, index] = value.astype(BF16)


def replay_state(accepted, path_dt, bias, a_log, conv_x, path_x, taps_x, conv_b, path_b, taps_b, state):
    seqs, heads, head_dim, state_dim = state.shape
    block = pl.BlockSpec((1, heads, head_dim, state_dim), lambda s: (s, 0, 0, 0))

    def full(array):
        return pl.BlockSpec(array.shape, lambda s: (0,) * array.ndim)

    small = [accepted, path_dt, bias, a_log, conv_x, path_x, taps_x, conv_b, path_b, taps_b]
    return pl.pallas_call(
        state_kernel,
        grid=(seqs,),
        out_shape=[
            jax.ShapeDtypeStruct(state.shape, F32),
            jax.ShapeDtypeStruct(state.shape, BF16),
        ],
        in_specs=[full(a) for a in small] + [block],
        out_specs=[block, block],
        scratch_shapes=[
            pltpu.VMEM((heads * head_dim, 2 * LANES), BF16),
            pltpu.VMEM((2 * LANES, path_b.shape[1]), F32),
            pltpu.VMEM((seqs, heads), F32),
        ],
        cost_estimate=cost(8),
        name="replay_state",
    )(*small, state)


def tree_kernel(parents_ref, accepted_ref, *refs):
    *inputs, links_ref, ancestry_ref, before_ref = refs
    seqs, props = parents_ref.shape
    nodes = seqs * props
    parents = parents_ref[...]
    parent = jnp.concatenate([parents[:, place : place + 1] for place in range(props)], axis=0)
    accepted = jnp.concatenate([as_column(accepted_ref[...])] * props, axis=0)
    row = lax.broadcasted_iota(jnp.int32, (nodes, nodes), 0)
    column = lax.broadcasted_iota(jnp.int32, (nodes, nodes), 1)
    own = lax.rem(lax.broadcasted_iota(jnp.int32, (nodes, 1), 0), seqs)
    target = jnp.where(parent >= 0, parent * seqs + own, -1)
    link = jnp.where(column == target, 1.0, 0.0)
    ancestry = link + jnp.where(row == column, 1.0, 0.0)
    link = link.astype(BF16)
    reach = link
    taps_count = inputs[2].shape[0]
    for distance in range(1, taps_count):
        links_ref[(distance - 1) * nodes : distance * nodes] = reach
        reach = dot(reach, link).astype(BF16)
    for _ in range(props.bit_length()):
        half = ancestry.astype(BF16)
        ancestry = jnp.minimum(dot(half, half), 1.0)
    ancestry_ref[...] = ancestry
    depth = jnp.sum(ancestry, axis=1, keepdims=True).astype(jnp.int32) - 1
    last = taps_count - 1

    def chosen(first, rows, distance):
        lane = lax.broadcasted_iota(jnp.int32, (nodes, rows), 1)
        wanted = accepted + last - distance + depth
        hit = (lane // seqs + first == wanted) & (lax.rem(lane, seqs) == own)
        return jnp.where(hit & (depth < distance), 1.0, 0.0).astype(BF16)

    conv_rows = inputs[0].shape[0]
    path_rows = inputs[1].shape[0]
    picks = [
        (chosen(0, conv_rows, d), chosen(conv_rows // seqs, path_rows, d))
        for d in range(1, taps_count)
    ]
    start = 0
    for which in range(0, len(inputs), 3):
        conv_ref, path_ref, taps_ref = inputs[which : which + 3]
        taps = taps_ref[...].astype(F32)
        total = 0.0
        for distance in range(1, taps_count):
            early, late = picks[distance - 1]
            found = dot(early, conv_ref[...]) + dot(late, path_ref[...])
            total = total + taps[last - distance : last - distance + 1] * found
        before_ref[:, start : start + conv_ref.shape[1]] = total
        start += conv_ref.shape[1]


def tree(parents, accepted, streams):
    nodes = parents.shape[0] * parents.shape[1]
    inputs = [array for stream in streams for array in stream]
    width = sum(stream[0].shape[1] for stream in streams)
    taps_count = streams[0][2].shape[0]
    return pl.pallas_call(
        tree_kernel,
        out_shape=[
            jax.ShapeDtypeStruct(((taps_count - 1) * nodes, nodes), BF16),
            jax.ShapeDtypeStruct((nodes, nodes), F32),
            jax.ShapeDtypeStruct((nodes, width), F32),
        ],
        in_specs=whole(len(inputs) + 2),
        out_specs=whole(3),
        cost_estimate=cost(4),
        name="tree",
    )(parents, accepted, *inputs)


def added(refs, span):
    return sum(ref[:, span].astype(F32) for ref in refs)


def mix_kernel(
    seqs,
    width,
    local_heads,
    addends,
    *refs,
):
    bcr_refs = refs[:addends]
    x_refs = refs[addends : 2 * addends]
    (
        links_ref,
        ancestry_ref,
        before_ref,
        taps_x_ref,
        taps_b_ref,
        taps_c_ref,
        bias_ref,
        a_log_ref,
        skip_ref,
        state_ref,
        extra_ref,
        out_ref,
        scale_ref,
        post_x_ref,
        post_b_ref,
        post_c_ref,
    ) = refs[2 * addends :]
    nodes, inner = x_refs[0].shape
    group_cols = taps_b_ref.shape[1]
    head_dim = inner // local_heads
    state_dim = state_ref.shape[3]
    groups = local_heads // HPG
    group_width = HPG * head_dim
    extra = extra_ref[...]
    empty = jnp.zeros((1, LANES - local_heads), F32)
    bias = jnp.concatenate([bias_ref[...], empty], axis=1)
    a_rate = jnp.concatenate([-jnp.exp(a_log_ref[...]), empty], axis=1)
    scale = lax.rsqrt(extra[:, local_heads : local_heads + 1] / width + EPS)
    scale_ref[...] = jnp.broadcast_to(scale, scale_ref.shape)

    ancestry = ancestry_ref[...]
    step = softplus((extra * scale).astype(BF16).astype(F32) + bias)
    decayed = step * a_rate
    high, rest = split(decayed)
    middle, low = split(rest)
    parts = jnp.concatenate([high, middle, low], axis=1).astype(BF16)
    parts = dot(ancestry.astype(BF16), parts)
    decay = parts[:, :LANES] + parts[:, LANES : 2 * LANES] + parts[:, 2 * LANES :]
    grow = jnp.exp(decay)
    decay_t = decay.T
    step_t = step.T
    is_live = ancestry > 0.5

    def convolve(row_refs, taps_ref, source, start, target_ref):
        last = taps_ref.shape[0] - 1
        for lower in range(0, taps_ref.shape[1], CHUNK):
            span = slice(lower, lower + CHUNK)
            rows = added(row_refs, slice(source + lower, source + lower + CHUNK))
            rows = (rows * scale).astype(BF16)
            taps = taps_ref[:, span].astype(F32)
            found = dot(links_ref[...], rows)
            total = before_ref[:, start + lower : start + lower + CHUNK]
            total = total + taps[last : last + 1] * rows.astype(F32)
            for distance in range(1, last + 1):
                total = total + taps[last - distance : last - distance + 1] * found[
                    (distance - 1) * nodes : distance * nodes
                ]
            target_ref[:, span] = silu(total).astype(target_ref.dtype)

    convolve(bcr_refs, taps_b_ref, 0, inner, post_b_ref)
    convolve(bcr_refs, taps_c_ref, group_cols, inner + group_cols, post_c_ref)
    convolve(x_refs, taps_x_ref, 0, 0, post_x_ref)

    own = lax.rem(lax.broadcasted_iota(jnp.int32, (nodes, 1), 0), seqs)
    per_lanes = LANES // head_dim
    lane_head = lax.broadcasted_iota(jnp.int32, (nodes, LANES), 1) // head_dim
    for group in range(groups):
        rows_c = post_c_ref[:, group * state_dim : (group + 1) * state_dim]
        rows_b = post_b_ref[:, group * state_dim : (group + 1) * state_dim]
        scores = dot_nt(rows_c, rows_b)
        wide_c = rows_c.astype(F32)
        carried = 0.0
        for sequence in range(0, seqs, 2):
            left = jnp.concatenate(
                [
                    jnp.where(own == sequence + place, wide_c, 0.0).astype(BF16)
                    for place in range(2)
                ],
                axis=1,
            )
            right = jnp.concatenate(
                [
                    state_ref[sequence + place, group * HPG : (group + 1) * HPG].reshape(
                        group_width, state_dim
                    )
                    for place in range(2)
                ],
                axis=1,
            )
            carried = carried + dot_nt(left, right)
        for part in range(group_width // LANES):
            start = group * group_width + part * LANES
            rows_x = post_x_ref[:, start : start + LANES]
            half_x = rows_x.astype(BF16)
            within = 0.0
            growth = 0.0
            skip = 0.0
            for place in range(per_lanes):
                head = group * HPG + part * per_lanes + place
                gap = decay[:, head : head + 1] - decay_t[head : head + 1, :nodes]
                mixing = jnp.where(is_live, jnp.exp(jnp.where(is_live, gap, 0.0)), 0.0)
                mixing = (scores * mixing * step_t[head : head + 1, :nodes]).astype(BF16)
                within = jnp.where(lane_head == place, dot(mixing, half_x), within)
                growth = jnp.where(lane_head == place, grow[:, head : head + 1], growth)
                skip = jnp.where(lane_head == place, skip_ref[:, head : head + 1], skip)
            out_ref[:, start : start + LANES] = (
                carried[:, part * LANES : (part + 1) * LANES] * growth
                + within
                + skip * rows_x
            )


def first_rows(arrays, nodes):
    return [pl.BlockSpec((nodes, array.shape[1]), lambda i: (0, 0)) for array in arrays]


def full_blocks(arrays):
    return [
        pl.BlockSpec(array.shape, functools.partial(lambda rank, i: (0,) * rank, array.ndim))
        for array in arrays
    ]


def mix(seqs, width, local_heads, bcr, x, others):
    nodes, inner = x[-1].shape
    group_cols = others[4].shape[1]
    outs = [
        jax.ShapeDtypeStruct((nodes, inner), F32),
        jax.ShapeDtypeStruct((nodes, LANES), F32),
    ]
    return pl.pallas_call(
        functools.partial(mix_kernel, seqs, width, local_heads, len(x)),
        grid=(1,),
        out_shape=outs,
        in_specs=first_rows(bcr + x, nodes) + full_blocks(others),
        out_specs=full_blocks(outs),
        scratch_shapes=[
            pltpu.VMEM((nodes, inner), F32),
            pltpu.VMEM((nodes, group_cols), BF16),
            pltpu.VMEM((nodes, group_cols), BF16),
        ],
        cost_estimate=cost(8),
        name="mix",
    )(*bcr, *x, *others)


def gate_kernel(group_width, *refs):
    *row_refs, scale_ref, heads_ref, gain_ref, out_ref = refs
    scale = scale_ref[:, :1]
    for lower in range(0, out_ref.shape[1], group_width):
        span = slice(lower, lower + group_width)
        rows = (added(row_refs, span) * scale).astype(BF16).astype(F32)
        gated = heads_ref[:, span] * silu(rows)
        mean = jnp.sum(gated * gated, axis=1, keepdims=True) / group_width
        out_ref[:, span] = (gated * lax.rsqrt(mean + EPS) * gain_ref[:, span]).astype(BF16)


def gate(group_width, rows, scale, heads_out, gain):
    out = jax.ShapeDtypeStruct(heads_out.shape, BF16)
    return pl.pallas_call(
        functools.partial(gate_kernel, group_width),
        grid=(1,),
        out_shape=out,
        in_specs=first_rows(rows, heads_out.shape[0]) + full_blocks([scale, heads_out, gain]),
        out_specs=full_blocks([out])[0],
        cost_estimate=cost(1),
        name="gate",
    )(*rows, scale, heads_out, gain)


def swap_bit(array, bit, blocks):
    return lax.ppermute(array, "kv", [(i, i ^ (1 << bit)) for i in range(blocks)])


def after(value, *others):
    return lax.optimization_barrier((value, *others))[0]


def halving(addends, bit, blocks, *others, axis=0):
    half = addends[-1].shape[axis] // 2
    addends = [*addends[:-1], after(addends[-1], *others)]
    send = sum(
        lax.slice_in_dim(addend, half, 2 * half, axis=axis).astype(F32)
        for addend in addends
    ).astype(BF16)
    return send, [*addends, swap_bit(send, bit, blocks)]


def mixer(
    kv_count,
    tp_count,
    tokens,
    parents,
    accepted,
    state,
    conv_x,
    conv_b,
    conv_c,
    path_x,
    path_b,
    path_c,
    path_dt,
    gain_in,
    w_x,
    w_z,
    w_b,
    w_c,
    w_dt,
    dt_bias,
    a_log,
    d_skip,
    conv_wx,
    conv_wb,
    conv_wc,
    gain_out,
    w_out,
):
    seq_local = state.shape[0]
    proposals = parents.shape[1]
    heads_local = dt_bias.shape[0]
    head_dim = state.shape[2]
    width = gain_in.shape[0]
    tp_index = lax.axis_index("tp")
    kv_index = lax.axis_index("kv")
    slab_width = tokens.shape[2]
    rows_local = seq_local * proposals
    z_count = tp_count
    x_count = kv_count // z_count
    x_bits = list(range(log2(x_count)))
    z_bits = list(range(log2(x_count), log2(kv_count)))
    x_first = x_bits + z_bits
    z_first = z_bits + x_bits
    z_place = kv_index // x_count

    def by_position(array):
        return array.transpose(1, 0, 2).reshape(-1, array.shape[2])

    tokens_q = tokens.transpose(1, 0, 2).reshape(proposals, kv_count, seq_local, slab_width)
    gains = gain_in[None, :]
    half = kv_count // 2
    of_x = [flipped_bits(position, x_first) for position in range(kv_count)]
    of_z = [flipped_bits(position, z_first) for position in range(kv_count)]
    w_dt_t = w_dt.T
    bcr_args = (tp_count, gains, [w_b, w_c], w_dt_t)
    x_args = (tp_count, gains, [w_x])
    z_args = (tp_count, gains, [w_z])
    send_bcr, send_rate = project(of_z[half:], tokens_q, *bcr_args)
    got_bcr = swap_bit(send_bcr, z_first[0], kv_count)
    (send_x,) = project(of_x[half:], after(tokens_q, send_bcr), *x_args)
    got_x = swap_bit(send_x, x_first[0], kv_count)
    (send_z,) = project(of_x[half:], after(tokens_q, send_x), *z_args)
    got_z = swap_bit(send_z, x_first[0], kv_count)
    got_rate = swap_bit(send_rate, z_first[0], kv_count)
    keep_bcr, keep_rate = project(of_z[:half], after(tokens_q, send_z), *bcr_args)
    (keep_x,) = project(of_x[:half], after(tokens_q, keep_bcr), *x_args)

    accepted = accepted[None, :]
    conv_x, conv_b, conv_c = by_position(conv_x), by_position(conv_b), by_position(conv_c)
    path_x, path_b, path_c = by_position(path_x), by_position(path_b), by_position(path_c)
    links, ancestry, before = tree(
        parents,
        after(accepted, keep_x),
        [(conv_x, path_x, conv_wx), (conv_b, path_b, conv_wb), (conv_c, path_c, conv_wc)],
    )
    sent_bcr, bcr = halving([keep_bcr, got_bcr], z_first[1], kv_count, links)
    sent_x, x = halving([keep_x, got_x], x_first[1], kv_count, sent_bcr)
    (keep_z,) = project(of_x[:half], after(tokens_q, sent_x), *z_args)
    sent_rate, rate = halving([keep_rate, got_rate], z_first[1], kv_count, keep_z, axis=1)
    new_state, half_state = replay_state(
        after(accepted, sent_rate),
        by_position(path_dt),
        dt_bias[None, :],
        a_log[None, :],
        conv_x,
        path_x,
        conv_wx,
        conv_b,
        path_b,
        conv_wb,
        state,
    )
    sent_z, z = halving([keep_z, got_z], x_first[1], kv_count, half_state)
    for place in range(2, len(x_first)):
        sent_x, x = halving(x, x_first[place], kv_count, sent_z)
        sent_bcr, bcr = halving(bcr, z_first[place], kv_count, sent_x)
        sent_rate, rate = halving(rate, z_first[place], kv_count, sent_bcr, axis=1)
        sent_z, z = halving(z, x_first[place], kv_count, sent_rate)

    rate[-1] = after(rate[-1], sent_z)
    extra = sum(addend[:, :rows_local].astype(F32) for addend in rate).T
    extra = jnp.pad(extra, ((0, 0), (0, LANES - RATE_ROWS)))
    heads_out, row_scale = mix(
        seq_local,
        width,
        heads_local,
        [*bcr[:-1], after(bcr[-1], sent_z)],
        [*x[:-1], after(x[-1], sent_z)],
        [
            links,
            ancestry,
            before,
            conv_wx,
            conv_wb,
            conv_wc,
            dt_bias[None, :],
            a_log[None, :],
            d_skip[None, :],
            half_state,
            extra,
        ],
    )
    gated = gate(HPG * head_dim, z, row_scale, heads_out, gain_out[None, :])

    w_out = after(w_out, sent_bcr, sent_x)
    w_pieces = [w_out]
    for bit in x_bits:
        w_pieces = w_pieces + [swap_bit(piece, bit, kv_count) for piece in w_pieces]
    w_pieces = [after(piece, gated) for piece in w_pieces]
    for bit in x_bits:
        flip = ((kv_index >> bit) & 1) == 1
        w_pieces = [
            jnp.where(flip, w_pieces[place ^ (1 << bit)], w_pieces[place])
            for place in range(x_count)
        ]
    w_block = jnp.concatenate(w_pieces, axis=1)

    pieces = {0: gated}
    for bit in z_bits[::-1]:
        for place in list(pieces):
            pieces[place | (1 << (bit - len(x_bits)))] = swap_bit(pieces[place], bit, kv_count)
    terms = [dot(pieces[place], w_block).astype(BF16) for place in range(z_count)]
    core_flip = ((tp_index ^ z_place) & 1) == 1
    sent = []
    kept = []
    for place in range(0, z_count, 2):
        sent.append(jnp.where(core_flip, terms[place], terms[place + 1]))
        kept.append(jnp.where(core_flip, terms[place + 1], terms[place]))
    swapped = lax.ppermute(
        jnp.concatenate(sent, axis=0), "tp", [(i, i ^ 1) for i in range(tp_count)]
    )
    half = z_count // 2
    paired = (jnp.concatenate(kept, axis=0).astype(F32) + swapped.astype(F32)).astype(
        BF16
    ).reshape(half, rows_local, -1)
    total = 0.0
    for shift in range(half):
        block = (tp_index >> 1) ^ (z_place >> 1) ^ shift
        route = []
        for z in range(z_count):
            for x in range(x_count):
                for t in range(tp_count):
                    z_to = (((t >> 1) ^ shift) << 1) | (t & 1)
                    route.append(
                        ((z * x_count + x) * tp_count + t, (z_to * x_count + x) * tp_count + z)
                    )
        piece = lax.dynamic_index_in_dim(paired, block, 0, keepdims=False)
        total = total + lax.ppermute(piece, ("kv", "tp"), route).astype(F32)
    mixed = total.astype(BF16).reshape(proposals, seq_local, -1).transpose(1, 0, 2)
    return (mixed, new_state)


def solution(mesh):
    return jax.shard_map(
        functools.partial(mixer, mesh.shape["kv"], mesh.shape["tp"]),
        mesh=mesh,
        in_specs=(
            P(None, None, "kv"),
            P("kv", None),
            P("kv"),
            P("kv", "tp", None, None),
            P("kv", None, "tp"),
            P("kv", None, "tp"),
            P("kv", None, "tp"),
            P("kv", None, "tp"),
            P("kv", None, "tp"),
            P("kv", None, "tp"),
            P("kv", None, "tp"),
            P(),
            P("kv", "tp"),
            P("kv", "tp"),
            P("kv", "tp"),
            P("kv", "tp"),
            P(),
            P("tp"),
            P("tp"),
            P("tp"),
            P(None, "tp"),
            P(None, "tp"),
            P(None, "tp"),
            P("tp"),
            P("tp", "kv"),
        ),
        out_specs=(P("kv", None, "tp"), P("kv", "tp", None, None)),
        check_vma=False,
    )
```

```python
import functools

import jax
import jax.numpy as jnp
from jax import lax
from jax.experimental import pallas as pl
from jax.experimental.pallas import tpu as pltpu
from jax.sharding import PartitionSpec as P


HPG = 4
EPS = 1e-06
LANES = 128
CHUNK = 256
RATE_ROWS = 32
VMEM = pltpu.VMEM
F32 = jnp.float32
BF16 = jnp.bfloat16
NT = (((1,), (1,)), ((), ()))


def log2(count):
    return count.bit_length() - 1


def flipped_bits(position, order):
    value = 0
    for place, bit in enumerate(order):
        value |= ((position >> (len(order) - 1 - place)) & 1) << bit
    return value


def whole(count):
    return [pl.BlockSpec(memory_space=VMEM) for _ in range(count)]


def cost(microseconds):
    return pl.CostEstimate(
        flops=int(microseconds * 4e6), bytes_accessed=1024, transcendentals=0
    )


def dot(left, right):
    return jnp.dot(left, right, preferred_element_type=F32)


def dot_nt(left, right):
    return lax.dot_general(left, right, NT, preferred_element_type=F32)


def silu(values):
    return values / (1.0 + jnp.exp(-values))


def softplus(values):
    return jnp.maximum(values, 0.0) + jnp.log1p(jnp.exp(-jnp.abs(values)))


def project_kernel(differences, with_rate, tp_count, tokens_ref, gain_ref, *refs):
    props, _, seqs, width = tokens_ref.shape
    me = lax.axis_index("kv")
    rows_local = props * seqs
    if with_rate:
        w_dt_ref, *w_refs, out_ref, rate_ref, scaled_ref, squares_ref, slab_ref, slab_sem = refs
    else:
        *w_refs, out_ref, scaled_ref = refs
    slab_start = pl.multiple_of(me * width, LANES)
    if with_rate:
        slab_copy = pltpu.make_async_copy(
            w_dt_ref.at[:, pl.ds(slab_start, width)], slab_ref, slab_sem
        )
        slab_copy.start()
    gain = gain_ref[:, pl.ds(slab_start, width)]
    for position, difference in enumerate(differences):
        rows = tokens_ref[:, me ^ difference].astype(F32).reshape(rows_local, width)
        span = slice(position * rows_local, (position + 1) * rows_local)
        scaled_ref[span] = (rows * gain).astype(BF16)
        if with_rate:
            high, low = split(rows * rows)
            squares_ref[0, span] = high.astype(BF16)
            squares_ref[1, span] = low.astype(BF16)
    start = 0
    for w_ref in w_refs:
        for lower in range(0, w_ref.shape[1], CHUNK):
            upper = min(lower + CHUNK, w_ref.shape[1])
            out_ref[:, start + lower : start + upper] = dot(
                scaled_ref[...], w_ref[:, lower:upper]
            ).astype(BF16)
        start += w_ref.shape[1]
    if with_rate:
        heads = w_dt_ref.shape[0]
        local = heads // tp_count
        first = lax.axis_index("tp") * local
        row = lax.broadcasted_iota(jnp.int32, (RATE_ROWS, heads), 0)
        column = lax.broadcasted_iota(jnp.int32, (RATE_ROWS, heads), 1)
        pick = jnp.where((row < local) & (column == row + first), 1.0, 0.0).astype(BF16)
        slab_copy.wait()
        w_rate = dot(pick, slab_ref[...]).astype(BF16)
        ones = jnp.ones((RATE_ROWS, width), BF16)
        squares = dot_nt(ones, squares_ref[0]) + dot_nt(ones, squares_ref[1])
        out_row = lax.broadcasted_iota(jnp.int32, (RATE_ROWS, 1), 0)
        rate = dot_nt(w_rate, scaled_ref[...])
        rate_ref[...] = jnp.where(out_row == local, squares, rate).astype(BF16)


def project(differences, tokens, tp_count, gain, weights, w_dt=None):
    props, _, seqs, width = tokens.shape
    rows = len(differences) * props * seqs
    columns = sum(weight.shape[1] for weight in weights)
    outs = [jax.ShapeDtypeStruct((rows, columns), BF16)]
    scratch = [pltpu.VMEM((rows, width), BF16)]
    operands = [tokens, gain]
    if w_dt is not None:
        outs.append(jax.ShapeDtypeStruct((RATE_ROWS, rows), BF16))
        scratch.append(pltpu.VMEM((2, rows, width), BF16))
        scratch.append(pltpu.VMEM((w_dt.shape[0], width), BF16))
        scratch.append(pltpu.SemaphoreType.DMA)
        operands.append(w_dt)
    operands += list(weights)
    specs = whole(len(operands))
    if w_dt is not None:
        specs[2] = pl.BlockSpec(memory_space=pl.ANY)
    return pl.pallas_call(
        functools.partial(project_kernel, tuple(differences), w_dt is not None, tp_count),
        out_shape=outs,
        in_specs=specs,
        out_specs=whole(len(outs)),
        scratch_shapes=scratch,
        cost_estimate=cost(2),
    )(*operands)


def window(conv_ref, path_ref, taps_ref, seqs):
    history = jnp.concatenate([conv_ref[...].astype(F32), path_ref[...].astype(F32)], axis=0)
    count = path_ref.shape[0]
    taps = taps_ref[...].astype(F32)
    total = taps[0:1] * history[0:count]
    for distance in range(1, taps.shape[0]):
        total = total + taps[distance : distance + 1] * history[
            distance * seqs : distance * seqs + count
        ]
    return silu(total)


def as_column(row):
    count = row.shape[1]
    place = lax.broadcasted_iota(jnp.int32, (count, count), 0)
    other = lax.broadcasted_iota(jnp.int32, (count, count), 1)
    return jnp.sum(jnp.where(place == other, row, 0), axis=1, keepdims=True)


def split(values):
    high = values.astype(BF16).astype(F32)
    return high, values - high


def state_kernel(
    accepted_ref,
    path_dt_ref,
    bias_ref,
    a_log_ref,
    conv_x_ref,
    path_x_ref,
    taps_x_ref,
    conv_b_ref,
    path_b_ref,
    taps_b_ref,
    state_ref,
    out_ref,
    half_ref,
    left_ref,
    right_ref,
    decay_ref,
):
    _, heads, head_dim, state_dim = state_ref.shape
    seqs = accepted_ref.shape[1]
    sequence = pl.program_id(0)
    count = path_x_ref.shape[0]
    group_width = HPG * head_dim

    @pl.when(sequence == 0)
    def _():
        lane = lax.broadcasted_iota(jnp.int32, (heads, heads * head_dim), 1)
        row = lax.broadcasted_iota(jnp.int32, (heads, heads * head_dim), 0)
        spread = jnp.where(lane // head_dim == row, 1.0, 0.0).astype(BF16)
        accepted = as_column(accepted_ref[...])
        a_rate = -jnp.exp(a_log_ref[...])
        steps = softplus(path_dt_ref[...].astype(F32) + bias_ref[...])
        weights = []
        overall = jnp.zeros((seqs, heads), F32)
        for position in range(count // seqs - 1, -1, -1):
            step = steps[position * seqs : (position + 1) * seqs]
            live = jnp.where(position < accepted, 1.0, 0.0)
            weights.append(live * jnp.exp(overall) * step)
            overall = overall + step * a_rate * live
        decay_ref[...] = jnp.exp(overall)
        high, low = split(jnp.concatenate(weights[::-1], axis=0))
        weights = dot(high.astype(BF16), spread) + dot(low.astype(BF16), spread)
        grown = weights * window(conv_x_ref, path_x_ref, taps_x_ref, seqs)
        empty = jnp.zeros((LANES - 2 * count, grown.shape[1]), F32)
        turned = jnp.concatenate([grown, grown, empty], axis=0).T
        high, low = split(turned)
        left_ref[:, :LANES] = high.astype(BF16)
        left_ref[:, LANES:] = low.astype(BF16)
        rows_b = window(conv_b_ref, path_b_ref, taps_b_ref, seqs)
        high, low = split(rows_b)
        right_ref[...] = jnp.zeros_like(right_ref)
        right_ref[0:count] = high
        right_ref[count : 2 * count] = low
        right_ref[LANES : LANES + count] = high

    row = lax.broadcasted_iota(jnp.int32, (2 * LANES, 1), 0)
    mine = jnp.where(lax.rem(row, seqs) == sequence, 1.0, 0.0)
    right = (right_ref[...] * mine).astype(BF16)
    decay = decay_ref[pl.ds(sequence, 1), :]
    for group in range(heads // HPG):
        grown = dot(
            left_ref[group * group_width : (group + 1) * group_width],
            right[:, group * state_dim : (group + 1) * state_dim],
        )
        for head in range(HPG):
            index = group * HPG + head
            value = decay[:, index : index + 1] * state_ref[0, index] + grown[
                head * head_dim : (head + 1) * head_dim
            ]
            out_ref[0, index] = value
            half_ref[0, index] = value.astype(BF16)


def replay_state(accepted, path_dt, bias, a_log, conv_x, path_x, taps_x, conv_b, path_b, taps_b, state):
    seqs, heads, head_dim, state_dim = state.shape
    block = pl.BlockSpec((1, heads, head_dim, state_dim), lambda s: (s, 0, 0, 0))

    def full(array):
        return pl.BlockSpec(array.shape, lambda s: (0,) * array.ndim)

    small = [accepted, path_dt, bias, a_log, conv_x, path_x, taps_x, conv_b, path_b, taps_b]
    return pl.pallas_call(
        state_kernel,
        grid=(seqs,),
        out_shape=[
            jax.ShapeDtypeStruct(state.shape, F32),
            jax.ShapeDtypeStruct(state.shape, BF16),
        ],
        in_specs=[full(a) for a in small] + [block],
        out_specs=[block, block],
        scratch_shapes=[
            pltpu.VMEM((heads * head_dim, 2 * LANES), BF16),
            pltpu.VMEM((2 * LANES, path_b.shape[1]), F32),
            pltpu.VMEM((seqs, heads), F32),
        ],
        cost_estimate=cost(8),
        name="replay_state",
    )(*small, state)


def tree_kernel(parents_ref, accepted_ref, *refs):
    *inputs, links_ref, ancestry_ref, before_ref = refs
    seqs, props = parents_ref.shape
    nodes = seqs * props
    parents = parents_ref[...]
    parent = jnp.concatenate([parents[:, place : place + 1] for place in range(props)], axis=0)
    accepted = jnp.concatenate([as_column(accepted_ref[...])] * props, axis=0)
    row = lax.broadcasted_iota(jnp.int32, (nodes, nodes), 0)
    column = lax.broadcasted_iota(jnp.int32, (nodes, nodes), 1)
    own = lax.rem(lax.broadcasted_iota(jnp.int32, (nodes, 1), 0), seqs)
    target = jnp.where(parent >= 0, parent * seqs + own, -1)
    link = jnp.where(column == target, 1.0, 0.0)
    ancestry = link + jnp.where(row == column, 1.0, 0.0)
    link = link.astype(BF16)
    reach = link
    taps_count = inputs[2].shape[0]
    for distance in range(1, taps_count):
        links_ref[(distance - 1) * nodes : distance * nodes] = reach
        reach = dot(reach, link).astype(BF16)
    for _ in range(props.bit_length()):
        half = ancestry.astype(BF16)
        ancestry = jnp.minimum(dot(half, half), 1.0)
    ancestry_ref[...] = ancestry
    depth = jnp.sum(ancestry, axis=1, keepdims=True).astype(jnp.int32) - 1
    last = taps_count - 1

    def chosen(first, rows, distance):
        lane = lax.broadcasted_iota(jnp.int32, (nodes, rows), 1)
        wanted = accepted + last - distance + depth
        hit = (lane // seqs + first == wanted) & (lax.rem(lane, seqs) == own)
        return jnp.where(hit & (depth < distance), 1.0, 0.0).astype(BF16)

    conv_rows = inputs[0].shape[0]
    path_rows = inputs[1].shape[0]
    picks = [
        (chosen(0, conv_rows, d), chosen(conv_rows // seqs, path_rows, d))
        for d in range(1, taps_count)
    ]
    start = 0
    for which in range(0, len(inputs), 3):
        conv_ref, path_ref, taps_ref = inputs[which : which + 3]
        taps = taps_ref[...].astype(F32)
        total = 0.0
        for distance in range(1, taps_count):
            early, late = picks[distance - 1]
            found = dot(early, conv_ref[...]) + dot(late, path_ref[...])
            total = total + taps[last - distance : last - distance + 1] * found
        before_ref[:, start : start + conv_ref.shape[1]] = total
        start += conv_ref.shape[1]


def tree(parents, accepted, streams):
    nodes = parents.shape[0] * parents.shape[1]
    inputs = [array for stream in streams for array in stream]
    width = sum(stream[0].shape[1] for stream in streams)
    taps_count = streams[0][2].shape[0]
    return pl.pallas_call(
        tree_kernel,
        out_shape=[
            jax.ShapeDtypeStruct(((taps_count - 1) * nodes, nodes), BF16),
            jax.ShapeDtypeStruct((nodes, nodes), F32),
            jax.ShapeDtypeStruct((nodes, width), F32),
        ],
        in_specs=whole(len(inputs) + 2),
        out_specs=whole(3),
        cost_estimate=cost(4),
        name="tree",
    )(parents, accepted, *inputs)


def added(refs, span):
    return sum(ref[:, span].astype(F32) for ref in refs)


def mix_kernel(
    seqs,
    width,
    local_heads,
    addends,
    *refs,
):
    bcr_refs = refs[:addends]
    x_refs = refs[addends : 2 * addends]
    (
        links_ref,
        ancestry_ref,
        before_ref,
        taps_x_ref,
        taps_b_ref,
        taps_c_ref,
        bias_ref,
        a_log_ref,
        skip_ref,
        state_ref,
        extra_ref,
        out_ref,
        scale_ref,
        post_x_ref,
        post_b_ref,
        post_c_ref,
    ) = refs[2 * addends :]
    nodes, inner = x_refs[0].shape
    group_cols = taps_b_ref.shape[1]
    head_dim = inner // local_heads
    state_dim = state_ref.shape[3]
    groups = local_heads // HPG
    group_width = HPG * head_dim
    extra = extra_ref[...]
    empty = jnp.zeros((1, LANES - local_heads), F32)
    bias = jnp.concatenate([bias_ref[...], empty], axis=1)
    a_rate = jnp.concatenate([-jnp.exp(a_log_ref[...]), empty], axis=1)
    scale = lax.rsqrt(extra[:, local_heads : local_heads + 1] / width + EPS)
    scale_ref[...] = jnp.broadcast_to(scale, scale_ref.shape)

    ancestry = ancestry_ref[...]
    step = softplus((extra * scale).astype(BF16).astype(F32) + bias)
    decayed = step * a_rate
    high, rest = split(decayed)
    middle, low = split(rest)
    parts = jnp.concatenate([high, middle, low], axis=1).astype(BF16)
    parts = dot(ancestry.astype(BF16), parts)
    decay = parts[:, :LANES] + parts[:, LANES : 2 * LANES] + parts[:, 2 * LANES :]
    grow = jnp.exp(decay)
    decay_t = decay.T
    step_t = step.T
    is_live = ancestry > 0.5

    def convolve(row_refs, taps_ref, source, start, target_ref):
        last = taps_ref.shape[0] - 1
        for lower in range(0, taps_ref.shape[1], CHUNK):
            span = slice(lower, lower + CHUNK)
            rows = added(row_refs, slice(source + lower, source + lower + CHUNK))
            rows = (rows * scale).astype(BF16)
            taps = taps_ref[:, span].astype(F32)
            found = dot(links_ref[...], rows)
            total = before_ref[:, start + lower : start + lower + CHUNK]
            total = total + taps[last : last + 1] * rows.astype(F32)
            for distance in range(1, last + 1):
                total = total + taps[last - distance : last - distance + 1] * found[
                    (distance - 1) * nodes : distance * nodes
                ]
            target_ref[:, span] = silu(total).astype(target_ref.dtype)

    convolve(bcr_refs, taps_b_ref, 0, inner, post_b_ref)
    convolve(bcr_refs, taps_c_ref, group_cols, inner + group_cols, post_c_ref)
    convolve(x_refs, taps_x_ref, 0, 0, post_x_ref)

    own = lax.rem(lax.broadcasted_iota(jnp.int32, (nodes, 1), 0), seqs)
    per_lanes = LANES // head_dim
    lane_head = lax.broadcasted_iota(jnp.int32, (nodes, LANES), 1) // head_dim
    for group in range(groups):
        rows_c = post_c_ref[:, group * state_dim : (group + 1) * state_dim]
        rows_b = post_b_ref[:, group * state_dim : (group + 1) * state_dim]
        scores = dot_nt(rows_c, rows_b)
        wide_c = rows_c.astype(F32)
        carried = 0.0
        for sequence in range(0, seqs, 2):
            left = jnp.concatenate(
                [
                    jnp.where(own == sequence + place, wide_c, 0.0).astype(BF16)
                    for place in range(2)
                ],
                axis=1,
            )
            right = jnp.concatenate(
                [
                    state_ref[sequence + place, group * HPG : (group + 1) * HPG].reshape(
                        group_width, state_dim
                    )
                    for place in range(2)
                ],
                axis=1,
            )
            carried = carried + dot_nt(left, right)
        for part in range(group_width // LANES):
            start = group * group_width + part * LANES
            rows_x = post_x_ref[:, start : start + LANES]
            half_x = rows_x.astype(BF16)
            within = 0.0
            growth = 0.0
            skip = 0.0
            for place in range(per_lanes):
                head = group * HPG + part * per_lanes + place
                gap = decay[:, head : head + 1] - decay_t[head : head + 1, :nodes]
                mixing = jnp.where(is_live, jnp.exp(jnp.where(is_live, gap, 0.0)), 0.0)
                mixing = (scores * mixing * step_t[head : head + 1, :nodes]).astype(BF16)
                within = jnp.where(lane_head == place, dot(mixing, half_x), within)
                growth = jnp.where(lane_head == place, grow[:, head : head + 1], growth)
                skip = jnp.where(lane_head == place, skip_ref[:, head : head + 1], skip)
            out_ref[:, start : start + LANES] = (
                carried[:, part * LANES : (part + 1) * LANES] * growth
                + within
                + skip * rows_x
            )


def first_rows(arrays, nodes):
    return [pl.BlockSpec((nodes, array.shape[1]), lambda i: (0, 0)) for array in arrays]


def full_blocks(arrays):
    return [
        pl.BlockSpec(array.shape, functools.partial(lambda rank, i: (0,) * rank, array.ndim))
        for array in arrays
    ]


def mix(seqs, width, local_heads, bcr, x, others):
    nodes, inner = x[-1].shape
    group_cols = others[4].shape[1]
    outs = [
        jax.ShapeDtypeStruct((nodes, inner), F32),
        jax.ShapeDtypeStruct((nodes, LANES), F32),
    ]
    return pl.pallas_call(
        functools.partial(mix_kernel, seqs, width, local_heads, len(x)),
        grid=(1,),
        out_shape=outs,
        in_specs=first_rows(bcr + x, nodes) + full_blocks(others),
        out_specs=full_blocks(outs),
        scratch_shapes=[
            pltpu.VMEM((nodes, inner), F32),
            pltpu.VMEM((nodes, group_cols), BF16),
            pltpu.VMEM((nodes, group_cols), BF16),
        ],
        cost_estimate=cost(8),
        name="mix",
    )(*bcr, *x, *others)


def gate_kernel(group_width, *refs):
    *row_refs, scale_ref, heads_ref, gain_ref, out_ref = refs
    scale = scale_ref[:, :1]
    for lower in range(0, out_ref.shape[1], group_width):
        span = slice(lower, lower + group_width)
        rows = (added(row_refs, span) * scale).astype(BF16).astype(F32)
        gated = heads_ref[:, span] * silu(rows)
        mean = jnp.sum(gated * gated, axis=1, keepdims=True) / group_width
        out_ref[:, span] = (gated * lax.rsqrt(mean + EPS) * gain_ref[:, span]).astype(BF16)


def gate(group_width, rows, scale, heads_out, gain):
    out = jax.ShapeDtypeStruct(heads_out.shape, BF16)
    return pl.pallas_call(
        functools.partial(gate_kernel, group_width),
        grid=(1,),
        out_shape=out,
        in_specs=first_rows(rows, heads_out.shape[0]) + full_blocks([scale, heads_out, gain]),
        out_specs=full_blocks([out])[0],
        cost_estimate=cost(1),
        name="gate",
    )(*rows, scale, heads_out, gain)


def swap_bit(array, bit, blocks):
    return lax.ppermute(array, "kv", [(i, i ^ (1 << bit)) for i in range(blocks)])


def after(value, *others):
    return lax.optimization_barrier((value, *others))[0]


def halving(addends, bit, blocks, *others, axis=0):
    half = addends[-1].shape[axis] // 2
    addends = [*addends[:-1], after(addends[-1], *others)]
    send = sum(
        lax.slice_in_dim(addend, half, 2 * half, axis=axis).astype(F32)
        for addend in addends
    ).astype(BF16)
    return send, [*addends, swap_bit(send, bit, blocks)]


def mixer(
    kv_count,
    tp_count,
    tokens,
    parents,
    accepted,
    state,
    conv_x,
    conv_b,
    conv_c,
    path_x,
    path_b,
    path_c,
    path_dt,
    gain_in,
    w_x,
    w_z,
    w_b,
    w_c,
    w_dt,
    dt_bias,
    a_log,
    d_skip,
    conv_wx,
    conv_wb,
    conv_wc,
    gain_out,
    w_out,
):
    seq_local = state.shape[0]
    proposals = parents.shape[1]
    heads_local = dt_bias.shape[0]
    head_dim = state.shape[2]
    width = gain_in.shape[0]
    tp_index = lax.axis_index("tp")
    kv_index = lax.axis_index("kv")
    slab_width = tokens.shape[2]
    rows_local = seq_local * proposals
    z_count = tp_count
    x_count = kv_count // z_count
    x_bits = list(range(log2(x_count)))
    z_bits = list(range(log2(x_count), log2(kv_count)))
    x_first = x_bits + z_bits
    z_first = z_bits + x_bits
    z_place = kv_index // x_count

    def by_position(array):
        return array.transpose(1, 0, 2).reshape(-1, array.shape[2])

    tokens_q = tokens.transpose(1, 0, 2).reshape(proposals, kv_count, seq_local, slab_width)
    gains = gain_in[None, :]
    half = kv_count // 2
    of_x = [flipped_bits(position, x_first) for position in range(kv_count)]
    of_z = [flipped_bits(position, z_first) for position in range(kv_count)]
    w_dt_t = w_dt.T
    bcr_args = (tp_count, gains, [w_b, w_c], w_dt_t)
    x_args = (tp_count, gains, [w_x])
    z_args = (tp_count, gains, [w_z])
    send_bcr, send_rate = project(of_z[half:], tokens_q, *bcr_args)
    got_bcr = swap_bit(send_bcr, z_first[0], kv_count)
    (send_x,) = project(of_x[half:], after(tokens_q, send_bcr), *x_args)
    got_x = swap_bit(send_x, x_first[0], kv_count)
    (send_z,) = project(of_x[half:], after(tokens_q, send_x), *z_args)
    got_z = swap_bit(send_z, x_first[0], kv_count)
    got_rate = swap_bit(send_rate, z_first[0], kv_count)
    keep_bcr, keep_rate = project(of_z[:half], after(tokens_q, send_z), *bcr_args)
    (keep_x,) = project(of_x[:half], after(tokens_q, keep_bcr), *x_args)

    accepted = accepted[None, :]
    conv_x, conv_b, conv_c = by_position(conv_x), by_position(conv_b), by_position(conv_c)
    path_x, path_b, path_c = by_position(path_x), by_position(path_b), by_position(path_c)
    links, ancestry, before = tree(
        parents,
        after(accepted, keep_x),
        [(conv_x, path_x, conv_wx), (conv_b, path_b, conv_wb), (conv_c, path_c, conv_wc)],
    )
    sent_bcr, bcr = halving([keep_bcr, got_bcr], z_first[1], kv_count, links)
    sent_x, x = halving([keep_x, got_x], x_first[1], kv_count, sent_bcr)
    (keep_z,) = project(of_x[:half], after(tokens_q, sent_x), *z_args)
    sent_rate, rate = halving([keep_rate, got_rate], z_first[1], kv_count, keep_z, axis=1)
    new_state, half_state = replay_state(
        after(accepted, sent_rate),
        by_position(path_dt),
        dt_bias[None, :],
        a_log[None, :],
        conv_x,
        path_x,
        conv_wx,
        conv_b,
        path_b,
        conv_wb,
        state,
    )
    sent_z, z = halving([keep_z, got_z], x_first[1], kv_count, half_state)
    for place in range(2, len(x_first)):
        sent_x, x = halving(x, x_first[place], kv_count, sent_z)
        sent_bcr, bcr = halving(bcr, z_first[place], kv_count, sent_x)
        sent_rate, rate = halving(rate, z_first[place], kv_count, sent_bcr, axis=1)
        sent_z, z = halving(z, x_first[place], kv_count, sent_rate)

    rate[-1] = after(rate[-1], sent_z)
    extra = sum(addend[:, :rows_local].astype(F32) for addend in rate).T
    extra = jnp.pad(extra, ((0, 0), (0, LANES - RATE_ROWS)))
    heads_out, row_scale = mix(
        seq_local,
        width,
        heads_local,
        [*bcr[:-1], after(bcr[-1], sent_z)],
        [*x[:-1], after(x[-1], sent_z)],
        [
            links,
            ancestry,
            before,
            conv_wx,
            conv_wb,
            conv_wc,
            dt_bias[None, :],
            a_log[None, :],
            d_skip[None, :],
            half_state,
            extra,
        ],
    )
    gated = gate(HPG * head_dim, z, row_scale, heads_out, gain_out[None, :])

    w_out = after(w_out, sent_bcr, sent_x)
    w_pieces = [w_out]
    for bit in x_bits:
        w_pieces = w_pieces + [swap_bit(piece, bit, kv_count) for piece in w_pieces]
    w_pieces = [after(piece, gated) for piece in w_pieces]
    for bit in x_bits:
        flip = ((kv_index >> bit) & 1) == 1
        w_pieces = [
            jnp.where(flip, w_pieces[place ^ (1 << bit)], w_pieces[place])
            for place in range(x_count)
        ]
    w_block = jnp.concatenate(w_pieces, axis=1)

    pieces = {0: gated}
    for bit in z_bits[::-1]:
        for place in list(pieces):
            pieces[place | (1 << (bit - len(x_bits)))] = swap_bit(pieces[place], bit, kv_count)
    terms = [dot(pieces[place], w_block).astype(BF16) for place in range(z_count)]
    core_flip = ((tp_index ^ z_place) & 1) == 1
    sent = []
    kept = []
    for place in range(0, z_count, 2):
        sent.append(jnp.where(core_flip, terms[place], terms[place + 1]))
        kept.append(jnp.where(core_flip, terms[place + 1], terms[place]))
    swapped = lax.ppermute(
        jnp.concatenate(sent, axis=0), "tp", [(i, i ^ 1) for i in range(tp_count)]
    )
    half = z_count // 2
    paired = (jnp.concatenate(kept, axis=0).astype(F32) + swapped.astype(F32)).astype(
        BF16
    ).reshape(half, rows_local, -1)
    total = 0.0
    for shift in range(half):
        block = (tp_index >> 1) ^ (z_place >> 1) ^ shift
        route = []
        for z in range(z_count):
            for x in range(x_count):
                for t in range(tp_count):
                    z_to = (((t >> 1) ^ shift) << 1) | (t & 1)
                    route.append(
                        ((z * x_count + x) * tp_count + t, (z_to * x_count + x) * tp_count + z)
                    )
        piece = lax.dynamic_index_in_dim(paired, block, 0, keepdims=False)
        total = total + lax.ppermute(piece, ("kv", "tp"), route).astype(F32)
    mixed = total.astype(BF16).reshape(proposals, seq_local, -1).transpose(1, 0, 2)
    return (mixed, new_state)


def solution(mesh):
    return jax.shard_map(
        functools.partial(mixer, mesh.shape["kv"], mesh.shape["tp"]),
        mesh=mesh,
        in_specs=(
            P(None, None, "kv"),
            P("kv", None),
            P("kv"),
            P("kv", "tp", None, None),
            P("kv", None, "tp"),
            P("kv", None, "tp"),
            P("kv", None, "tp"),
            P("kv", None, "tp"),
            P("kv", None, "tp"),
            P("kv", None, "tp"),
            P("kv", None, "tp"),
            P(),
            P("kv", "tp"),
            P("kv", "tp"),
            P("kv", "tp"),
            P("kv", "tp"),
            P(),
            P("tp"),
            P("tp"),
            P("tp"),
            P(None, "tp"),
            P(None, "tp"),
            P(None, "tp"),
            P("tp"),
            P("tp", "kv"),
        ),
        out_specs=(P("kv", None, "tp"), P("kv", "tp", None, None)),
        check_vma=False,
    )
```
